32 devices in a mesh: sp: 8 (over z, x), tp: 4 (over y, core).
Axes of the slice: x: 2, y: 2, z: 4, core: 2. Of those that a mesh axis runs over, the one named last changes fastest.
Arguments:
- conv_out: bfloat16 [1536, 2048], P('sp', 'tp'), may hold values from -6 to 6
- gate_in: bfloat16 [1536, 2048], P('sp', 'tp'), may hold values from -6 to 6
- block_states: float32 [8, 2048], P('sp', 'tp'), may hold values from -4 to 4
- decay_param: float32 [2048], P('tp'), may hold values from 4 to 20
- decay_shift: float32 [1536], P('sp'), may hold values from -2 to 0, as said below
- w_reset: bfloat16 [16, 128, 128], P('tp'), may hold values from -0.5 to 0.5
- w_input: bfloat16 [16, 128, 128], P('tp'), may hold values from -0.5 to 0.5
- w_out: bfloat16 [2048, 2048], P('tp'), may hold values from -0.125 to 0.125
- mixed: bfloat16 [1536, 2048], P('sp', 'tp'), may hold values from -6 to 6
- d_out: bfloat16 [1536, 2048], P('sp', 'tp'), may hold values from -6 to 6
- expert_ids: int32 [1536, 2], P('sp'), may hold values from 0 to 7, all different within a row; in each aligned block of 192 rows (0 to 191, 192 to 383, ...) at most 96 rows name the same one
- route_weights: float32 [1536, 2], P('sp'), may hold values from 0.2 to 1.4
- w_gate: bfloat16 [8, 2048, 1024], P('sp', None, 'tp'), may hold values from -0.125 to 0.125
- w_up: bfloat16 [8, 2048, 1024], P('sp', None, 'tp'), may hold values from -0.125 to 0.125
- w_down: bfloat16 [8, 1024, 2048], P('sp', 'tp'), may hold values from -0.1875 to 0.1875
Outputs:
- grad_w_gate: float32 [8, 2048, 1024], P('sp', None, 'tp')
- grad_w_up: float32 [8, 2048, 1024], P('sp', None, 'tp')
- grad_w_down: float32 [8, 1024, 2048], P('sp', 'tp')
- grad_out_proj_t: float32 [2048, 2048], P('sp', 'tp')
- recurrence_input_gradient: bfloat16 [1536, 2048], P('sp', 'tp')
- grad_gate: bfloat16 [1536, 2048], P('sp', 'tp')
The draws below stay inside these ranges and needn't reach their ends.
Inputs may be any that keep to these rules, and one draw needn't show every extreme that they name: `expert_ids`: each row names 2 different experts; among the 192 tokens of one index of sp no expert is named more than 96 times, and in some index of sp one expert is named exactly 96 times. decay_shift is at most -0.05 / 1536 at every position.
All inputs are finite; a program needn't handle non-finite values.
Results may differ from the reference program's by a relative error of at most 0.013.
Values may be sent and summed in bfloat16 or wider, within the bound.
A program may use at most 128 MiB of HBM per device.

```python
import math
import jax
import jax.numpy as jnp
import numpy as np
from jax import lax

D = 2048
HEADS = 16
HEAD_DIM = 128
DR = 2048
FE = 1024
TOP = 2
TOK_DEV = 192
SEQUENCE_TOKENS = 1536
EXPERTS = 8
CAP = 96
N_SP = 8
N_TP = 4


def draw_decay_param(key, part):
    chooser, slow_key, fast_key = jax.random.split(jax.random.fold_in(key, 11), 3)
    portion = 0.5
    is_slow = jax.random.uniform(chooser, (DR,), jnp.float32) < portion
    slow_rate = jax.random.uniform(slow_key, (DR,), jnp.float32, minval=0.1, maxval=0.4) / (4.0 * SEQUENCE_TOKENS)
    fast_rate = 1.0 / (4.0 * jax.random.uniform(fast_key, (DR,), jnp.float32, minval=30.0, maxval=100.0))
    rates = jnp.where(is_slow, slow_rate, fast_rate)
    return (-jnp.log(jnp.expm1(rates))).astype(jnp.float32)


def draw_decay_shift(key, part):
    level_key, location_key, depth_key = jax.random.split(jax.random.fold_in(key, 23), 3)
    blocks = SEQUENCE_TOKENS // TOK_DEV
    levels = jnp.exp(jax.random.uniform(level_key, (blocks,), jnp.float32, minval=math.log(0.05), maxval=math.log(0.4)))
    reference_value = -jnp.repeat(levels, TOK_DEV) / SEQUENCE_TOKENS
    spike_locations = jax.random.randint(location_key, (2,), 0, SEQUENCE_TOKENS)
    nesting_levels = jax.random.uniform(depth_key, (2,), jnp.float32, minval=math.log(0.6), maxval=math.log(0.8))
    return reference_value.at[spike_locations].add(nesting_levels).astype(jnp.float32)


def raised(entries, key, source, target, blocks, factor):
    owner, partner = [(jnp.arange(entries.shape[position]) // (entries.shape[position] // blocks)).reshape([-1 if axis == position else 1 for axis in range(entries.ndim)]) for position in (source, target)]
    chosen = jax.random.permutation(key, blocks)[partner]
    strong = (owner == chosen) | (owner == (partner + blocks // 2) % blocks)
    return jnp.where(strong, factor * entries, entries)


def shard_levels(key, extent, cuts, smallest, high):
    def one(axis_at, parts):
        draws = jax.random.uniform(jax.random.fold_in(jax.random.fold_in(key, 6), axis_at), (parts,), jnp.float32, smallest / len(cuts), high / len(cuts))
        return jnp.repeat(jnp.exp(draws), extent[axis_at] // parts).reshape((-1,) + (1,) * (len(extent) - axis_at - 1))

    gain = one(*cuts[0])
    for cut in cuts[1:]:
        gain = gain * one(*cut)
    return gain


def assign_block(own_key, own, number, rows, count, top, limit, lean):
    ranking = jax.random.permutation(own_key, count)
    packed, ordinary = portions_of(count, rows * top, limit, lean, True), portions_of(count, rows * top, limit, lean, False)
    places = jnp.arange(count)

    def named(lengths, offset_by):
        used = int((lengths > 0).sum())
        fixed = max(1, used // 4)
        passed = fixed + (places - fixed + offset_by * (used - fixed)) % max(1, count - fixed)
        return jnp.zeros((count,), jnp.int32).at[ranking[jnp.where(places < fixed, places, passed)]].set(jnp.asarray(lengths, jnp.int32))

    lengths = jnp.where(number % 4 == 0, named(packed, number // 4), named(ordinary, number - number // 4 - 1))
    mixed = jax.random.permutation(jax.random.fold_in(own, 3), count)
    giver, sink = mixed[0:count // 2 * 2:2], mixed[1:count // 2 * 2:2]
    margin = jnp.minimum(lengths[giver] - 1, limit - lengths[sink]) // 2
    margin = jnp.where((giver == ranking[0]) | (sink == ranking[0]) | (lengths[sink] == 0), 0, jnp.maximum(margin, 0))
    passed = jax.random.randint(jax.random.fold_in(own, 4), (count // 2,), 0, 1 << 20) % (margin + 1)
    lengths = lengths.at[giver].add(-passed).at[sink].add(passed)
    items = jnp.searchsorted(jnp.cumsum(lengths), jnp.arange(rows * top), side="right").astype(jnp.int32)
    listing = items.reshape(top, rows).T
    listing = listing[jax.random.permutation(jax.random.fold_in(own, 1), rows)]
    offset_by = jax.random.randint(jax.random.fold_in(own, 2), (rows, 1), 0, top)
    return jnp.take_along_axis(listing, (jnp.arange(top)[None, :] + offset_by) % top, axis=1)


def portions_of(count, total, limit, lean, full):
    weights = [(1 << 20) // math.isqrt(grade ** lean) + 1 for grade in range(1, count + 1)]
    largest = limit if full else min(limit, max(-(-total // count), total * weights[0] // sum(weights)))
    least = 1 if total - largest >= count - 1 else 0
    given, rest = [largest] + [least] * (count - 1), total - largest - least * (count - 1)
    while rest > 0:
        candidates = [i for i in range(1, count) if given[i] < largest] or [i for i in range(1, count) if given[i] < limit]
        whole, left = sum([weights[i] for i in candidates]), rest
        for i in candidates:
            more = min(limit - given[i], max(1, left * weights[i] // whole), rest)
            given[i] = given[i] + more
            rest = rest - more
    return np.array(given)


def bell_draw(own_key, shape, width, bound, cuts=(), kind=jnp.bfloat16):
    drawn = jax.random.normal(own_key, shape, jnp.float32) * width
    if len(cuts) > 0:
        drawn = shard_levels(own_key, shape, cuts, -0.22, 0.18) * drawn
    return jnp.clip(drawn, min=-bound, max=bound).astype(kind)


def noise_with(own_key, extent, width, most, shards, heavy, kind=jnp.bfloat16):
    result = width * jax.random.normal(own_key, extent, jnp.float32)
    if shards:
        result = result * shard_levels(own_key, extent, shards, -0.22, 0.18)
    return jnp.clip(raised(result, jax.random.fold_in(own_key, 3), *heavy), -most, most).astype(kind)


def setup_inputs(seed: int = 0) -> dict:
    key_list = jax.random.split(jax.random.key(seed), 16)
    conv_out = bell_draw(key_list[0], (SEQUENCE_TOKENS, DR), 1.0, 6.0, ((0, 8), (1, 4)))
    gate_in = bell_draw(key_list[1], (SEQUENCE_TOKENS, DR), 1.0, 6.0, ((0, 8), (1, 4)))
    block_states = bell_draw(key_list[2], (N_SP, DR), 0.5, 4.0, ((0, 8), (1, 4)), jnp.float32)
    decay_param = draw_decay_param(jax.random.fold_in(key_list[15], 71), 0)
    decay_shift = draw_decay_shift(jax.random.fold_in(key_list[15], 71), 0)
    w_reset = bell_draw(key_list[5], (HEADS, HEAD_DIM, HEAD_DIM), HEAD_DIM ** -0.5, 0.5, ((0, 4),))
    w_input = bell_draw(key_list[6], (HEADS, HEAD_DIM, HEAD_DIM), HEAD_DIM ** -0.5, 0.5, ((0, 4),))
    w_out = bell_draw(key_list[7], (DR, D), DR ** -0.5, 0.125, ((0, 4),))
    mixed = bell_draw(key_list[8], (SEQUENCE_TOKENS, D), 1.0, 6.0, ((0, 8), (1, 4)))
    d_out = noise_with(key_list[9], (SEQUENCE_TOKENS, D), 1.0, 6.0, ((0, 8), (1, 4)), (0, 1, 8, 2.0))
    expert_ids_keys = jax.random.split(jax.random.fold_in(key_list[10], 1), SEQUENCE_TOKENS // TOK_DEV)
    expert_ids_turns = jax.random.permutation(jax.random.fold_in(key_list[10], 3), SEQUENCE_TOKENS // TOK_DEV)
    expert_ids = jax.vmap(lambda own, number: assign_block(jax.random.fold_in(key_list[10], 2), own, number, TOK_DEV, EXPERTS, TOP, CAP, 1))(expert_ids_keys, expert_ids_turns).reshape((SEQUENCE_TOKENS, TOP))
    route_weights = jnp.clip(0.2 + 1.19999997 * jax.random.uniform(key_list[11], (SEQUENCE_TOKENS, TOP), jnp.float32) ** shard_levels(key_list[11], (SEQUENCE_TOKENS, TOP), ((0, 8),), -0.2, 0.2), 0.2, 1.4)
    w_gate = bell_draw(key_list[12], (EXPERTS, D, FE), D ** -0.5, 0.125, ((0, 8), (2, 4)))
    w_up = bell_draw(key_list[13], (EXPERTS, D, FE), D ** -0.5, 0.125, ((0, 8), (2, 4)))
    w_down = bell_draw(key_list[14], (EXPERTS, FE, D), FE ** -0.5, 0.1875, ((0, 8), (1, 4)))
    return dict(conv_out=conv_out, gate_in=gate_in, block_states=block_states, decay_param=decay_param, decay_shift=decay_shift, w_reset=w_reset, w_input=w_input, w_out=w_out, mixed=mixed, d_out=d_out, expert_ids=expert_ids, route_weights=route_weights, w_gate=w_gate, w_up=w_up, w_down=w_down)


def decay_combine(first_pair, second_pair):
    return (first_pair[0] * second_pair[0], second_pair[0] * first_pair[1] + second_pair[1])

def gelu_slope(values):
    outcome, pullback = jax.vjp(jax.nn.gelu, values)
    return (outcome, pullback(jnp.ones_like(values))[0])

def head_maps(values, weights):
    count = values.shape[0]
    split = values.astype(jnp.float32).reshape(count, weights.shape[0], weights.shape[1])
    mapped = jnp.einsum('thi,hij->thj', split, weights.astype(jnp.float32))
    return mapped.reshape(count, -1)

def head_back(grads, weights):
    count = grads.shape[0]
    split = grads.astype(jnp.float32).reshape(count, weights.shape[0], weights.shape[2])
    mapped = jnp.einsum('thj,hij->thi', split, weights.astype(jnp.float32))
    return mapped.reshape(count, -1)

def over_rows(left_matrix, right_matrix):
    return lax.dot_general(left_matrix, right_matrix, (((0,), (0,)), ((), ())), preferred_element_type=jnp.float32)

def against_rows(left_matrix, right_matrix):
    return lax.dot_general(left_matrix, right_matrix, (((1,), (1,)), ((), ())), preferred_element_type=jnp.float32)

def reference(conv_out, gate_in, block_states, decay_param, decay_shift, w_reset, w_input, w_out, mixed, d_out, expert_ids, route_weights, w_gate, w_up, w_down):
    conv_full = conv_out.astype(jnp.float32)
    reset = jax.nn.sigmoid(head_maps(conv_out, w_reset))
    input_gate = jax.nn.sigmoid(head_maps(conv_out, w_input))
    slow_rate = jax.nn.softplus(-decay_param)
    log_decay = -8.0 * reset * slow_rate[None, :] + decay_shift[:, None]
    decays = jnp.exp(log_decay)
    norm_in = jnp.sqrt(-jnp.expm1(2.0 * log_decay))
    drives = norm_in * input_gate * conv_full
    blocked = (N_SP, TOK_DEV, DR)
    cum_decay, cum_drive = lax.associative_scan(decay_combine, (decays.reshape(blocked), drives.reshape(blocked)), axis=1)
    states = cum_decay * block_states[:, None, :] + cum_drive
    prev_states = jnp.concatenate([block_states[:, None, :], states[:, :-1]], axis=1).reshape(SEQUENCE_TOKENS, DR)
    states = states.reshape(SEQUENCE_TOKENS, DR)
    gate_act, gate_deriv = gelu_slope(gate_in.astype(jnp.float32))
    merged_in = (gate_act * states).astype(jnp.bfloat16)
    flat_ids = expert_ids.reshape(N_SP, TOK_DEV * TOP)
    onehot = (flat_ids[:, :, None] == jnp.arange(EXPERTS, dtype=jnp.int32)[None, None, :]).astype(jnp.int32)
    slot_rank = lax.optimization_barrier(jnp.sum((jnp.cumsum(onehot, axis=1) - 1) * onehot, axis=2))
    source_index = jnp.arange(N_SP, dtype=jnp.int32)[:, None]
    slot_flat = (source_index * CAP + slot_rank).reshape(-1).astype(jnp.int32)
    expert_flat = expert_ids.reshape(-1).astype(jnp.int32)
    assign_ids = jnp.arange(SEQUENCE_TOKENS * TOP, dtype=jnp.int32)
    slot_table = jnp.full((EXPERTS, N_SP * CAP), SEQUENCE_TOKENS * TOP, jnp.int32).at[expert_flat, slot_flat].set(assign_ids)
    scaled_cot = (route_weights[:, :, None] * d_out.astype(jnp.float32)[:, None, :]).astype(jnp.bfloat16).reshape(SEQUENCE_TOKENS * TOP, D)
    cot_padded = jnp.concatenate([scaled_cot, jnp.zeros((1, D), jnp.bfloat16)], axis=0)
    mixed_padded = jnp.concatenate([mixed, jnp.zeros((1, D), jnp.bfloat16)], axis=0)
    block_width = FE // N_TP

    def one_expert(operands):
        slot_ids, gate_matrix, up_matrix, down_matrix = operands
        token_ids = jnp.where(slot_ids < SEQUENCE_TOKENS * TOP, slot_ids // TOP, SEQUENCE_TOKENS)
        expert_in = mixed_padded[token_ids]
        expert_cot = cot_padded[slot_ids]
        up_pre = jnp.dot(expert_in, gate_matrix, preferred_element_type=jnp.float32)
        linear = jnp.dot(expert_in, up_matrix, preferred_element_type=jnp.float32)
        sigmoid_up = jax.nn.sigmoid(up_pre)
        silu_up = up_pre * sigmoid_up
        hidden_state = (silu_up * linear).astype(jnp.bfloat16)
        d_hidden = against_rows(expert_cot, down_matrix)
        d_linear = (d_hidden * silu_up).astype(jnp.bfloat16)
        d_up = (d_hidden * linear * sigmoid_up * (1.0 + up_pre * (1.0 - sigmoid_up))).astype(jnp.bfloat16)
        grad_gate_e = over_rows(expert_in, d_up)
        grad_up_e = over_rows(expert_in, d_linear)
        grad_down_e = over_rows(hidden_state, expert_cot)
        row_count = expert_in.shape[0]
        up_blocks = d_up.astype(jnp.float32).reshape(row_count, N_TP, block_width)
        lin_blocks = d_linear.astype(jnp.float32).reshape(row_count, N_TP, block_width)
        gate_blocks = gate_matrix.astype(jnp.float32).reshape(D, N_TP, block_width)
        upw_blocks = up_matrix.astype(jnp.float32).reshape(D, N_TP, block_width)
        pieces = jnp.einsum('rqf,dqf->qrd', up_blocks, gate_blocks) + jnp.einsum('rqf,dqf->qrd', lin_blocks, upw_blocks)
        rounded = lax.optimization_barrier(pieces.astype(jnp.bfloat16))
        row_grad = lax.optimization_barrier(jnp.sum(rounded.astype(jnp.float32), axis=0)).astype(jnp.bfloat16)
        return (grad_gate_e, grad_up_e, grad_down_e, row_grad)
    grad_w_gate, grad_w_up, grad_w_down, row_grads = lax.map(one_expert, (slot_table, w_gate, w_up, w_down))
    returned = row_grads[expert_flat, slot_flat].astype(jnp.float32).reshape(SEQUENCE_TOKENS, TOP, D)
    d_mixed = (d_out.astype(jnp.float32) + lax.optimization_barrier(jnp.sum(returned, axis=1))).astype(jnp.bfloat16)
    grad_out_proj_t = over_rows(d_mixed, merged_in)
    d_merged = against_rows(d_mixed, w_out)
    grad_gate = (d_merged * states * gate_deriv).astype(jnp.bfloat16)
    d_states = d_merged * gate_act
    next_decay = jnp.concatenate([decays[1:], jnp.zeros((1, DR), jnp.float32)], axis=0)
    _, state_flipped = lax.associative_scan(decay_combine, (next_decay[::-1], d_states[::-1]), axis=0)
    state_grad = state_flipped[::-1]
    d_log_decay = state_grad * decays * prev_states - state_grad * input_gate * conv_full * decays * decays / norm_in
    d_pre_reset = (d_log_decay * (-8.0 * slow_rate[None, :]) * reset * (1.0 - reset)).astype(jnp.bfloat16)
    d_pre_input = (state_grad * norm_in * conv_full * input_gate * (1.0 - input_gate)).astype(jnp.bfloat16)
    recurrence_input_gradient = (state_grad * norm_in * input_gate + head_back(d_pre_reset, w_reset) + head_back(d_pre_input, w_input)).astype(jnp.bfloat16)
    return (grad_w_gate, grad_w_up, grad_w_down, grad_out_proj_t, recurrence_input_gradient, grad_gate)
```

```python
import functools
import jax
import jax.numpy as jnp
from jax import lax
from jax.experimental import pallas as pl
from jax.experimental.pallas import tpu as pltpu
from jax.sharding import PartitionSpec as P

MESH = pl.DeviceIdType.MESH
GELU_C = 0.7978845608028654
GELU_K = 0.044715


def gelu_both(x):
    inner = jnp.tanh(GELU_C * (x + GELU_K * x * x * x))
    act = 0.5 * x * (1.0 + inner)
    slope = 0.5 * (1.0 + inner) + 0.5 * x * (1.0 - inner * inner) * (
        GELU_C * (1.0 + 3.0 * GELU_K * x * x)
    )
    return act, slope


def recurrence_forward(
    conv_ref, gate_ref, bs_ref, slow, shift, wr_ref, wi_ref,
    merged_ref, reset_ref, inp_ref, dec_ref, norm_ref, st_ref, prev_ref, drive,
):
    rows = conv_ref.shape[0]
    width = wr_ref.shape[1]
    for h in range(wr_ref.shape[0]):
        cols = slice(h * width, (h + 1) * width)
        conv = conv_ref[:, cols]
        reset = jax.nn.sigmoid(jnp.dot(conv, wr_ref[h], preferred_element_type=jnp.float32))
        inp = jax.nn.sigmoid(jnp.dot(conv, wi_ref[h], preferred_element_type=jnp.float32))
        log_decay = -8.0 * reset * slow[:, cols] + shift
        decays = jnp.exp(log_decay)
        norm = jnp.sqrt(-jnp.tanh(log_decay) * (decays * decays + 1.0))
        reset_ref[:, cols] = reset
        inp_ref[:, cols] = inp
        dec_ref[:, cols] = decays
        norm_ref[:, cols] = norm
        drive[:, cols] = norm * inp * conv.astype(jnp.float32)
    total = conv_ref.shape[1]
    row = lax.broadcasted_iota(jnp.int32, (8, total), 0)
    carry = bs_ref[...]
    for i in range(rows // 8):
        at = slice(8 * i, 8 * i + 8)
        a = dec_ref[at, :]
        b = drive[at, :]
        for d in (1, 2, 4):
            b = b + a * jnp.where(row >= d, pltpu.roll(b, d, 0), 0.0)
            a = a * jnp.where(row >= d, pltpu.roll(a, d, 0), 1.0)
        state = a * carry + b
        st_ref[at, :] = state
        prev_ref[at, :] = jnp.where(row >= 1, pltpu.roll(state, 1, 0), carry)
        carry = state[7:8, :]
    for h in range(wr_ref.shape[0]):
        cols = slice(h * width, (h + 1) * width)
        x = gate_ref[:, cols].astype(jnp.float32)
        inner = jnp.tanh(GELU_C * (x + GELU_K * x * x * x))
        merged_ref[:, cols] = (0.5 * x * (1.0 + inner) * st_ref[:, cols]).astype(jnp.bfloat16)


def backward_kernel(
    n, dm_ref, wo_ref, conv_ref, gate_ref, slow_ref, reset_ref, inp_ref, dec_ref, norm_ref,
    st_ref, prev_ref, wr_ref, wi_ref, blocks_ref,
    out_ref, gg_ref, got_ref,
    grad, prods, dstate, mine_pair, pairs, send_sem, recv_sem, block_send, block_recv,
):
    me = lax.axis_index("sp")
    barrier = pltpu.get_barrier_semaphore()
    for off in range(1, n):
        pl.semaphore_signal(
            barrier, inc=1, device_id={"sp": lax.rem(me + off, n)}, device_id_type=MESH
        )
    rows = conv_ref.shape[0]
    width = wr_ref.shape[1]
    total = conv_ref.shape[1]
    heads = wr_ref.shape[0]
    dstate[...] = lax.dot_general(
        dm_ref[...], wo_ref[...], (((1,), (1,)), ((), ())), preferred_element_type=jnp.float32
    )
    pl.semaphore_wait(barrier, n - 1)

    def block_to(peer, source):
        return pltpu.make_async_remote_copy(
            src_ref=blocks_ref.at[peer],
            dst_ref=got_ref.at[source],
            send_sem=block_send.at[0],
            recv_sem=block_recv.at[source],
            device_id={"sp": peer},
            device_id_type=MESH,
        )

    keep = pltpu.make_async_copy(blocks_ref.at[me], got_ref.at[me], block_send.at[1])
    keep.start()
    for off in range(1, n):
        block_to(lax.rem(me + off, n), me).start()
    for h in range(heads):
        cols = slice(h * width, (h + 1) * width)
        act, slope = gelu_both(gate_ref[:, cols].astype(jnp.float32))
        d_merged = dstate[:, cols]
        gg_ref[:, cols] = (d_merged * st_ref[:, cols] * slope).astype(jnp.bfloat16)
        dstate[:, cols] = d_merged * act
    row = lax.broadcasted_iota(jnp.int32, (8, total), 0)
    carry_g = jnp.zeros((1, total), jnp.float32)
    carry_p = jnp.ones((1, total), jnp.float32)
    following = jnp.ones((1, total), jnp.float32)
    for i in reversed(range(rows // 8)):
        at = slice(8 * i, 8 * i + 8)
        decay = dec_ref[at, :]
        a = jnp.where(row < 7, pltpu.roll(decay, 7, 0), following)
        following = decay[0:1, :]
        b = dstate[at, :]
        for d in (1, 2, 4):
            b = b + a * jnp.where(row < 8 - d, pltpu.roll(b, 8 - d, 0), 0.0)
            a = a * jnp.where(row < 8 - d, pltpu.roll(a, 8 - d, 0), 1.0)
        g = a * carry_g + b
        p = a * carry_p
        grad[at, :] = g
        prods[at, :] = p
        carry_g = g[0:1, :]
        carry_p = p[0:1, :]
    mine_pair[0:1, :] = carry_p * following
    mine_pair[1:2, :] = carry_g * following
    mine_pair[2:8, :] = jnp.zeros((6, total), jnp.float32)
    pairs[me] = jnp.zeros((8, total), jnp.float32)

    def copy_to(peer, source):
        return pltpu.make_async_remote_copy(
            src_ref=mine_pair,
            dst_ref=pairs.at[source],
            send_sem=send_sem.at[0],
            recv_sem=recv_sem.at[source],
            device_id={"sp": peer},
            device_id_type=MESH,
        )

    for off in range(1, n):
        copy_to(lax.rem(me + off, n), me).start()
    for off in range(1, n):
        copy_to(lax.rem(me + off, n), lax.rem(me + off, n)).wait_recv()
    for off in range(1, n):
        copy_to(lax.rem(me + off, n), me).wait_send()
    enter = jnp.zeros((1, total), jnp.float32)
    for p in reversed(range(n)):
        pair = pairs[p]
        enter = jnp.where(p > me, pair[1:2, :] + pair[0:1, :] * enter, enter)
    for h in range(heads):
        cols = slice(h * width, (h + 1) * width)
        state_grad = grad[:, cols] + prods[:, cols] * enter[:, cols]
        conv = conv_ref[:, cols].astype(jnp.float32)
        inp, norm = inp_ref[:, cols], norm_ref[:, cols]
        decays, reset = dec_ref[:, cols], reset_ref[:, cols]
        d_log = state_grad * decays * prev_ref[:, cols] - (
            state_grad * inp * conv * decays * decays / norm
        )
        d_r = (d_log * (-8.0 * slow_ref[:, cols]) * reset * (1.0 - reset)).astype(jnp.bfloat16)
        d_i = (state_grad * norm * conv * inp * (1.0 - inp)).astype(jnp.bfloat16)
        out_ref[:, cols] = (
            state_grad * norm * inp
            + lax.dot_general(d_r, wr_ref[h], (((1,), (1,)), ((), ())), preferred_element_type=jnp.float32)
            + lax.dot_general(d_i, wi_ref[h], (((1,), (1,)), ((), ())), preferred_element_type=jnp.float32)
        ).astype(jnp.bfloat16)
    keep.wait()
    for off in range(1, n):
        peer = lax.rem(me + off, n)
        block_to(peer, peer).wait_recv()
        block_to(peer, me).wait_send()


VM = pl.BlockSpec(memory_space=pltpu.VMEM)


def run_backward(n, *args):
    shape = args[2].shape
    half = jax.ShapeDtypeStruct(shape, jnp.bfloat16)
    return pl.pallas_call(
        functools.partial(backward_kernel, n),
        out_shape=(half, half, jax.ShapeDtypeStruct(args[-1].shape, jnp.bfloat16)),
        in_specs=[VM] * len(args),
        out_specs=(VM, VM, pl.BlockSpec(memory_space=pl.ANY)),
        scratch_shapes=[pltpu.VMEM(shape, jnp.float32)] * 3
        + [
            pltpu.VMEM((8, shape[1]), jnp.float32),
            pltpu.VMEM((n, 8, shape[1]), jnp.float32),
            pltpu.SemaphoreType.DMA((1,)),
            pltpu.SemaphoreType.DMA((n,)),
            pltpu.SemaphoreType.DMA((2,)),
            pltpu.SemaphoreType.DMA((n,)),
        ],
        compiler_params=pltpu.CompilerParams(collective_id=0, has_side_effects=True),
        cost_estimate=pl.CostEstimate(flops=400_000_000, bytes_accessed=40_000_000, transcendentals=0),
    )(*args)


def softplus_of_negative(x):
    small = jnp.exp(-jnp.abs(x))
    ratio = small / (2.0 + small)
    square = ratio * ratio
    series = jnp.zeros_like(x)
    for odd in range(17, 0, -2):
        series = series * square + 1.0 / odd
    return jnp.maximum(-x, 0.0) + 2.0 * ratio * series


def front_kernel(
    n, groups,
    mixed_ref, cot_ref, ids_ref, wts_ref,
    conv_ref, gate_ref, bs_ref, param_ref, shift_ref, wr_ref, wi_ref,
    wg_hbm, wu_hbm, wd_hbm,
    gg_hbm, gu_hbm, gd_hbm, dm_ref,
    merged_ref, slow_ref, reset_ref, inp_ref, dec_ref, norm_ref, st_ref, prev_ref,
    wg, wu, wd, send, xbuf, dbuf, hbuf, pbuf, nbuf, sbuf, fbuf, rbuf, ret, dcols, dmbuf,
    acc_g, acc_u, acc_d, drive,
    send_sem, sp_sem, y_sem, own_sem, fwd_sem, near_sem, far_sem, ret_sem, dm_sem, w_sem, g_sem,
):
    me, q = lax.axis_index("sp"), lax.axis_index("tp")
    near, far = q ^ 1, q ^ 2
    barrier = pltpu.get_barrier_semaphore()
    for off in range(1, n):
        pl.semaphore_signal(
            barrier, inc=1, device_id={"sp": lax.rem(me + off, n)}, device_id_type=MESH
        )
    for other in (near, far):
        pl.semaphore_signal(barrier, inc=1, device_id={"tp": other}, device_id_type=MESH)
    loads = [
        pltpu.make_async_copy(src, dst, w_sem.at[i])
        for i, (src, dst) in enumerate(((wg_hbm, wg), (wu_hbm, wu), (wd_hbm, wd)))
    ]
    for copy in loads:
        copy.start()
    tokens, width = mixed_ref.shape
    top = ids_ref.shape[1]
    slots = send.shape[2]
    hidden = wg.shape[1]
    parts = xbuf.shape[0]
    per = n // groups
    block = per * slots

    lanes = 128
    lane = lax.broadcasted_iota(jnp.int32, (tokens, lanes), 1)
    away = []
    for j in range(top):
        gap = ids_ref[:, j : j + 1] - me
        away.append(jnp.where(gap < 0, gap + n, gap))
    member = jnp.zeros((tokens, lanes), jnp.float32)
    for j in range(top):
        member = jnp.where(away[j] == lane, 1.0, member)
    earlier = lax.broadcasted_iota(jnp.int32, (tokens, tokens), 1) < (
        lax.broadcasted_iota(jnp.int32, (tokens, tokens), 0)
    )
    rank = jnp.dot(
        jnp.where(earlier, 1.0, 0.0).astype(jnp.bfloat16),
        member.astype(jnp.bfloat16),
        preferred_element_type=jnp.float32,
    )
    place = lax.broadcasted_iota(jnp.int32, (tokens, n * slots), 1)
    picks = []
    for j in range(top):
        mine = jnp.sum(jnp.where(away[j] == lane, rank, 0.0), axis=1, keepdims=True)
        at = away[j] * slots + mine.astype(jnp.int32)
        picks.append(jnp.where(place == at, 1.0, 0.0).astype(jnp.bfloat16))
    pick_all = picks[0]
    for j in range(1, top):
        pick_all = pick_all + picks[j]

    def over(left, right):
        return lax.dot_general(
            left, right, (((0,), (0,)), ((), ())), preferred_element_type=jnp.float32
        )

    def against(left, right):
        return lax.dot_general(
            left, right, (((1,), (1,)), ((), ())), preferred_element_type=jnp.float32
        )

    send[:, 0] = over(pick_all, mixed_ref[...]).astype(jnp.bfloat16).reshape(n, slots, width)
    chosen = jnp.zeros((n * slots, width), jnp.float32)
    for j in range(top):
        scaled = wts_ref[:, j : j + 1] * cot_ref[...].astype(jnp.float32)
        chosen = chosen + over(picks[j], scaled.astype(jnp.bfloat16))
    send[:, 1] = chosen.astype(jnp.bfloat16).reshape(n, slots, width)
    sent = []

    def remote(src, dst, recv, where):
        return pltpu.make_async_remote_copy(
            src_ref=src, dst_ref=dst, send_sem=send_sem.at[0], recv_sem=recv,
            device_id=where, device_id_type=MESH,
        )

    def start(copy):
        copy.start()
        sent.append(copy)

    def over_sp(k):
        return remote(
            send.at[k], xbuf.at[q, k], sp_sem.at[k], {"sp": lax.rem(me + k, n)}
        )

    def over_tp(owner, k, other, sems):
        spot = xbuf.at[owner, k]
        return remote(spot, spot, sems.at[k], {"tp": other})

    def spread(k):
        if k > 0:
            over_sp(k).wait_recv()
        start(over_tp(q, k, far, y_sem))
        start(over_tp(q, k, near, own_sem))

    def relay(k):
        over_tp(far, k, far, y_sem).wait_recv()
        start(over_tp(far, k, near, fwd_sem))

    def near_copy(g, i):
        return remote(
            pbuf.at[g, near if i == 0 else far ^ 1], nbuf.at[g, i], near_sem.at[g, i], {"tp": near}
        )

    def expert(g):
        ks = range(g * per, (g + 1) * per)
        for k in ks:
            over_tp(near, k, near, own_sem).wait_recv()
            over_tp(near ^ 2, k, near, fwd_sem).wait_recv()
        here = slice(g * per, (g + 1) * per)
        up_pre = jnp.zeros((block, hidden), jnp.float32)
        linear = jnp.zeros((block, hidden), jnp.float32)
        d_hidden = jnp.zeros((block, hidden), jnp.float32)
        for b in range(parts):
            cols = slice(b * width, (b + 1) * width)
            x = xbuf[b, here, 0].reshape(block, width)
            c = xbuf[b, here, 1].reshape(block, width)
            up_pre += jnp.dot(x, wg[cols, :], preferred_element_type=jnp.float32)
            linear += jnp.dot(x, wu[cols, :], preferred_element_type=jnp.float32)
            d_hidden += against(c, wd[:, cols])
        sig = jax.nn.sigmoid(up_pre)
        silu = up_pre * sig
        rows = slice(g * block, (g + 1) * block)
        hbuf[rows, :] = (silu * linear).astype(jnp.bfloat16)
        d_linear = (d_hidden * silu).astype(jnp.bfloat16)
        d_up = (d_hidden * linear * sig * (1.0 + up_pre * (1.0 - sig))).astype(jnp.bfloat16)
        dbuf[rows, :hidden] = d_up
        dbuf[rows, hidden:] = d_linear
        for b in range(parts):
            cols = slice(b * width, (b + 1) * width)
            pbuf[g, b] = (against(d_up, wg[cols, :]) + against(d_linear, wu[cols, :])).astype(
                jnp.bfloat16
            )
        for i in range(2):
            start(near_copy(g, 1 - i))

    def far_copy(g):
        return remote(sbuf.at[g], fbuf.at[g], far_sem.at[g], {"tp": far})

    def join_near(g):
        near_copy(g, 1).wait_recv()
        sbuf[g] = (pbuf[g, far].astype(jnp.float32) + nbuf[g, 1].astype(jnp.float32)).astype(
            jnp.bfloat16
        )
        start(far_copy(g))

    def back_copy(g, i):
        k = g * per + i
        return remote(
            rbuf.at[g, i], ret.at[k], ret_sem.at[k], {"sp": lax.rem(me + n - k, n)}
        )

    def join_far(g):
        near_copy(g, 0).wait_recv()
        far_copy(g).wait_recv()
        whole = (
            pbuf[g, q].astype(jnp.float32)
            + nbuf[g, 0].astype(jnp.float32)
            + fbuf[g].astype(jnp.float32)
        )
        rbuf[g] = whole.astype(jnp.bfloat16).reshape(per, slots, width)
        for i in range(per):
            if g * per + i > 0:
                start(back_copy(g, i))
        if g == 0:
            ret[0] = whole[:slots].astype(jnp.bfloat16)

    g_copies = []

    def grads(h):
        half = n // 2
        here = slice(h * half, (h + 1) * half)
        rows = slice(h * half * slots, (h + 1) * half * slots)
        d_both = dbuf[rows, :]
        hid = hbuf[rows, :]
        for b in range(parts):
            cols = slice(b * width, (b + 1) * width)
            x = xbuf[b, here, 0].reshape(half * slots, width)
            c = xbuf[b, here, 1].reshape(half * slots, width)
            both = over(x, d_both)
            down = over(hid, c)
            if h == 0:
                acc_g[cols, :] = both[:, :hidden]
                acc_u[cols, :] = both[:, hidden:]
                acc_d[:, cols] = down
            else:
                acc_g[cols, :] += both[:, :hidden]
                acc_u[cols, :] += both[:, hidden:]
                acc_d[:, cols] += down
        if h == 1:
            for i, (src, dst) in enumerate(((acc_g, gg_hbm), (acc_u, gu_hbm), (acc_d, gd_hbm))):
                copy = pltpu.make_async_copy(src, dst, g_sem.at[i])
                copy.start()
                g_copies.append(copy)

    pl.semaphore_wait(barrier, n + 1)
    for k in range(1, n):
        start(over_sp(k))
    xbuf[q, 0] = send[0]
    spread(0)
    slow = softplus_of_negative(param_ref[...])
    slow_ref[...] = slow
    eye = lax.broadcasted_iota(jnp.int32, (tokens, tokens), 0) == (
        lax.broadcasted_iota(jnp.int32, (tokens, tokens), 1)
    )
    shift = jnp.sum(jnp.where(eye, shift_ref[...], 0.0), axis=1, keepdims=True)
    recurrence_forward(
        conv_ref, gate_ref, bs_ref, slow, shift, wr_ref, wi_ref,
        merged_ref, reset_ref, inp_ref, dec_ref, norm_ref, st_ref, prev_ref, drive,
    )
    for copy in loads:
        copy.wait()
    done = 0
    for k in range(1, n + 1):
        if k < n:
            spread(k)
        relay(k - 1)
        ready = (k - 1) // per
        if k >= per + 1 and (k - 1) % per == 0:
            g = ready - 1
            expert(g)
            if g >= 1:
                join_near(g - 1)
            if g >= 2:
                join_far(g - 2)
            if g == groups // 2 - 1:
                pass
    last = groups - 1
    expert(last)
    join_near(last - 1)
    join_far(last - 2)
    join_near(last)
    grads(0)
    join_far(last - 1)
    join_far(last)
    grads(1)
    for k in range(1, n):
        back_copy(k // per, k % per).wait_recv()
    summed = jnp.dot(
        pick_all, ret[...].reshape(n * slots, width), preferred_element_type=jnp.float32
    )
    dcols[...] = (cot_ref[...].astype(jnp.float32) + summed).astype(jnp.bfloat16)

    def dm_copy(owner, i, other, src):
        return remote(src, dmbuf.at[owner], dm_sem.at[i], {"tp": other})

    start(dm_copy(q, 0, far, dcols))
    start(dm_copy(q, 1, near, dcols))
    dmbuf[q] = dcols[...]
    dm_copy(far, 0, far, dcols).wait_recv()
    start(dm_copy(far, 2, near, dmbuf.at[far]))
    dm_copy(near, 1, near, dcols).wait_recv()
    dm_copy(near ^ 2, 2, near, dcols).wait_recv()
    for b in range(parts):
        dm_ref[:, b * width : (b + 1) * width] = dmbuf[b]
    for copy in g_copies:
        copy.wait()
    for copy in sent:
        copy.wait_send()


def run_front(n, parts, slots, mixed, cot, ids, weights, conv, gate, bs, param, shift, wr, wi, wg, wu, wd):
    tokens, width = mixed.shape
    full, hidden = wg.shape
    groups = 4
    per = n // groups
    block = per * slots
    half = jnp.bfloat16
    anywhere = pl.BlockSpec(memory_space=pl.ANY)
    dma = pltpu.SemaphoreType.DMA
    f32 = jnp.float32
    wide = jax.ShapeDtypeStruct((tokens, width), f32)
    vm = pltpu.VMEM
    return pl.pallas_call(
        functools.partial(front_kernel, n, groups),
        out_shape=(
            jax.ShapeDtypeStruct((full, hidden), f32),
            jax.ShapeDtypeStruct((full, hidden), f32),
            jax.ShapeDtypeStruct((hidden, full), f32),
            jax.ShapeDtypeStruct((tokens, full), half),
            jax.ShapeDtypeStruct((tokens, width), half),
            jax.ShapeDtypeStruct((1, width), f32),
        ) + (wide,) * 6,
        in_specs=[VM] * 11 + [anywhere] * 3,
        out_specs=(anywhere,) * 3 + (VM,) * 9,
        scratch_shapes=[
            vm((full, hidden), half), vm((full, hidden), half), vm((hidden, full), half),
            vm((n, 2, slots, width), half),
            vm((parts, n, 2, slots, width), half),
            vm((n * slots, 2 * hidden), half), vm((n * slots, hidden), half),
            vm((groups, parts, block, width), half),
            vm((groups, 2, block, width), half),
            vm((groups, block, width), half),
            vm((groups, block, width), half),
            vm((groups, per, slots, width), half),
            vm((n, slots, width), half),
            vm((tokens, width), half),
            vm((parts, tokens, width), half),
            vm((full, hidden), f32), vm((full, hidden), f32), vm((hidden, full), f32),
            vm((tokens, width), f32),
            dma((1,)), dma((n,)), dma((n,)), dma((n,)), dma((n,)), dma((groups, 2)),
            dma((groups,)), dma((n,)), dma((3,)), dma((3,)), dma((3,)),
        ],
        compiler_params=pltpu.CompilerParams(
            collective_id=1, has_side_effects=True, vmem_limit_bytes=60 * 1024 * 1024
        ),
        cost_estimate=pl.CostEstimate(flops=8_000_000_000, bytes_accessed=80_000_000, transcendentals=0),
    )(mixed, cot, ids, weights, conv, gate, bs, param, shift, wr, wi, wg, wu, wd)


def over_rows(left_matrix, right_matrix):
    return lax.dot_general(
        left_matrix, right_matrix, (((0,), (0,)), ((), ())), preferred_element_type=jnp.float32
    )


def body(
    conv_out, gate_in, block_states, decay_param, decay_shift, w_reset, w_input, w_out,
    mixed, d_out, expert_ids, route_weights, w_gate, w_up, w_down,
):
    tok_rows, top_k = expert_ids.shape
    experts = lax.axis_size("sp")
    capacity = 2 * tok_rows * top_k // experts
    slots = -(-capacity // 16) * 16
    (
        grad_gate_e, grad_up_e, grad_down_e, d_mixed,
        merged_in, slow_rate, reset, input_gate, decays, norm_in, states, prev_states,
    ) = run_front(
        experts, lax.axis_size("tp"), slots, mixed, d_out, expert_ids, route_weights,
        conv_out, gate_in, block_states, decay_param[None, :], decay_shift[None, :],
        w_reset, w_input, w_gate[0], w_up[0], w_down[0],
    )
    merged_full = lax.all_gather(merged_in, "sp", axis=0, tiled=True)
    blocks = d_mixed.reshape(tok_rows, experts, -1).transpose(1, 0, 2)
    recurrence_input_gradient, grad_gate, got_blocks = run_backward(
        experts, d_mixed, w_out, conv_out, gate_in, slow_rate, reset, input_gate, decays, norm_in,
        states, prev_states, w_reset, w_input, blocks,
    )
    grad_out_proj_t = over_rows(got_blocks.reshape(experts * tok_rows, -1), merged_full)
    return (
        grad_gate_e[None],
        grad_up_e[None],
        grad_down_e[None],
        grad_out_proj_t,
        recurrence_input_gradient,
        grad_gate,
    )


def solution(mesh):
    placed = (
        P("sp", "tp"),
        P("sp", "tp"),
        P("sp", "tp"),
        P("tp"),
        P("sp"),
        P("tp", None, None),
        P("tp", None, None),
        P("tp", None),
        P("sp", "tp"),
        P("sp", "tp"),
        P("sp", None),
        P("sp", None),
        P("sp", None, "tp"),
        P("sp", None, "tp"),
        P("sp", "tp", None),
    )
    return jax.shard_map(
        body,
        mesh=mesh,
        in_specs=placed,
        out_specs=(
            P("sp", None, "tp"),
            P("sp", None, "tp"),
            P("sp", "tp", None),
            P("sp", "tp"),
            P("sp", "tp"),
            P("sp", "tp"),
        ),
        check_vma=False,
    )
```

```python
import functools
import jax
import jax.numpy as jnp
from jax import lax
from jax.experimental import pallas as pl
from jax.experimental.pallas import tpu as pltpu
from jax.sharding import PartitionSpec as P

MESH = pl.DeviceIdType.MESH
GELU_C = 0.7978845608028654
GELU_K = 0.044715


def gelu_both(x):
    inner = jnp.tanh(GELU_C * (x + GELU_K * x * x * x))
    act = 0.5 * x * (1.0 + inner)
    slope = 0.5 * (1.0 + inner) + 0.5 * x * (1.0 - inner * inner) * (
        GELU_C * (1.0 + 3.0 * GELU_K * x * x)
    )
    return act, slope


def softplus_of_negative(x):
    small = jnp.exp(-jnp.abs(x))
    ratio = small / (2.0 + small)
    square = ratio * ratio
    series = jnp.zeros_like(x)
    for odd in range(17, 0, -2):
        series = series * square + 1.0 / odd
    return jnp.maximum(-x, 0.0) + 2.0 * ratio * series


def whole_kernel(
    n, groups,
    mixed_ref, cot_ref, ids_ref, wts_ref,
    conv_ref, gate_ref, bs_ref, param_ref, shift_ref, wr_ref, wi_ref,
    wg_hbm, wu_hbm, wd_hbm, wo_hbm,
    gg_hbm, gu_hbm, gd_hbm, go_ref, out_ref, gate_out_ref,
    wg, wu, wd, wo, send, xbuf, dbuf, hbuf, pbuf, nbuf, sbuf, fbuf, rbuf, ret, dcols, dmbuf,
    acc_g, acc_u, acc_d, dec, drive, st, act_b, slope_b, fac_r, fac_i, fac_o, prods, lev0, lev1, lev2, grad,
    mg, got, bsend, mine_pair, pairs,
    send_sem, sp_sem, y_sem, own_sem, fwd_sem, near_sem, far_sem, ret_sem, dm_sem, w_sem, g_sem,
    mz_sem, mx_sem, blk_sem, got_sem, pair_sem,
):
    me, q = lax.axis_index("sp"), lax.axis_index("tp")
    near, far = q ^ 1, q ^ 2
    barrier = pltpu.get_barrier_semaphore()
    for off in range(1, n):
        pl.semaphore_signal(
            barrier, inc=1, device_id={"sp": lax.rem(me + off, n)}, device_id_type=MESH
        )
    for other in (near, far):
        pl.semaphore_signal(barrier, inc=1, device_id={"tp": other}, device_id_type=MESH)
    loads = [
        pltpu.make_async_copy(src, dst, w_sem.at[i])
        for i, (src, dst) in enumerate(((wg_hbm, wg), (wu_hbm, wu), (wd_hbm, wd), (wo_hbm, wo)))
    ]
    for copy in loads:
        copy.start()
    tokens, width = mixed_ref.shape
    top = ids_ref.shape[0]
    slots = send.shape[2]
    hidden = wg.shape[1]
    parts = xbuf.shape[0]
    per = n // groups
    block = per * slots
    heads, head_dim = wr_ref.shape[0], wr_ref.shape[1]
    f32, half = jnp.float32, jnp.bfloat16

    eye = lax.broadcasted_iota(jnp.int32, (tokens, tokens), 0) == (
        lax.broadcasted_iota(jnp.int32, (tokens, tokens), 1)
    )

    def upright(row):
        return jnp.sum(jnp.where(eye, row, jnp.zeros_like(row)), axis=1, keepdims=True)

    lanes = 128
    lane = lax.broadcasted_iota(jnp.int32, (tokens, lanes), 1)
    away = []
    for j in range(top):
        gap = upright(ids_ref[j : j + 1, :].astype(f32)).astype(jnp.int32) - me
        away.append(jnp.where(gap < 0, gap + n, gap))
    member = jnp.zeros((tokens, lanes), f32)
    for j in range(top):
        member = jnp.where(away[j] == lane, 1.0, member)
    earlier = lax.broadcasted_iota(jnp.int32, (tokens, tokens), 1) < (
        lax.broadcasted_iota(jnp.int32, (tokens, tokens), 0)
    )
    rank = jnp.dot(
        jnp.where(earlier, 1.0, 0.0).astype(half), member.astype(half), preferred_element_type=f32
    )
    place = lax.broadcasted_iota(jnp.int32, (tokens, n * slots), 1)
    picks = []
    for j in range(top):
        mine = jnp.sum(jnp.where(away[j] == lane, rank, 0.0), axis=1, keepdims=True)
        at = away[j] * slots + mine.astype(jnp.int32)
        picks.append(jnp.where(place == at, 1.0, 0.0).astype(half))
    pick_all = picks[0]
    for j in range(1, top):
        pick_all = pick_all + picks[j]

    def over(left, right):
        return lax.dot_general(left, right, (((0,), (0,)), ((), ())), preferred_element_type=f32)

    def against(left, right):
        return lax.dot_general(left, right, (((1,), (1,)), ((), ())), preferred_element_type=f32)

    send[:, 0] = over(pick_all, mixed_ref[...]).astype(half).reshape(n, slots, width)
    chosen = jnp.zeros((n * slots, width), f32)
    for j in range(top):
        scaled = upright(wts_ref[j : j + 1, :]) * cot_ref[...].astype(f32)
        chosen = chosen + over(picks[j], scaled.astype(half))
    send[:, 1] = chosen.astype(half).reshape(n, slots, width)
    sent = []

    def remote(src, dst, recv, where):
        return pltpu.make_async_remote_copy(
            src_ref=src, dst_ref=dst, send_sem=send_sem.at[0], recv_sem=recv,
            device_id=where, device_id_type=MESH,
        )

    def start(copy):
        copy.start()
        sent.append(copy)

    def over_sp(k):
        return remote(send.at[k], xbuf.at[q, k], sp_sem.at[k], {"sp": lax.rem(me + k, n)})

    def over_tp(owner, k, other, sems):
        spot = xbuf.at[owner, k]
        return remote(spot, spot, sems.at[k], {"tp": other})

    def spread(k):
        if k > 0:
            over_sp(k).wait_recv()
        start(over_tp(q, k, far, y_sem))
        start(over_tp(q, k, near, own_sem))

    def relay(k):
        over_tp(far, k, far, y_sem).wait_recv()
        start(over_tp(far, k, near, fwd_sem))

    def near_copy(g, i):
        return remote(
            pbuf.at[g, near if i == 0 else far ^ 1], nbuf.at[g, i], near_sem.at[g, i], {"tp": near}
        )

    def expert(g):
        for k in range(g * per, (g + 1) * per):
            over_tp(near, k, near, own_sem).wait_recv()
            over_tp(near ^ 2, k, near, fwd_sem).wait_recv()
        here = slice(g * per, (g + 1) * per)
        up_pre = jnp.zeros((block, hidden), f32)
        linear = jnp.zeros((block, hidden), f32)
        d_hidden = jnp.zeros((block, hidden), f32)
        for b in range(parts):
            cols = slice(b * width, (b + 1) * width)
            x = xbuf[b, here, 0].reshape(block, width)
            c = xbuf[b, here, 1].reshape(block, width)
            up_pre += jnp.dot(x, wg[cols, :], preferred_element_type=f32)
            linear += jnp.dot(x, wu[cols, :], preferred_element_type=f32)
            d_hidden += against(c, wd[:, cols])
        sig = jax.nn.sigmoid(up_pre)
        silu = up_pre * sig
        rows = slice(g * block, (g + 1) * block)
        hbuf[rows, :] = (silu * linear).astype(half)
        d_linear = (d_hidden * silu).astype(half)
        d_up = (d_hidden * linear * sig * (1.0 + up_pre * (1.0 - sig))).astype(half)
        dbuf[rows, :hidden] = d_up
        dbuf[rows, hidden:] = d_linear
        for b in range(parts):
            cols = slice(b * width, (b + 1) * width)
            pbuf[g, b] = (against(d_up, wg[cols, :]) + against(d_linear, wu[cols, :])).astype(half)
        for i in range(2):
            start(near_copy(g, 1 - i))

    def far_copy(g):
        return remote(sbuf.at[g], fbuf.at[g], far_sem.at[g], {"tp": far})

    def join_near(g):
        near_copy(g, 1).wait_recv()
        sbuf[g] = (pbuf[g, far].astype(f32) + nbuf[g, 1].astype(f32)).astype(half)
        start(far_copy(g))

    def back_copy(g, i):
        k = g * per + i
        return remote(
            rbuf.at[g, i], ret.at[k], ret_sem.at[k], {"sp": lax.rem(me + n - k, n)}
        )

    def join_far(g):
        near_copy(g, 0).wait_recv()
        far_copy(g).wait_recv()
        whole = pbuf[g, q].astype(f32) + nbuf[g, 0].astype(f32) + fbuf[g].astype(f32)
        rbuf[g] = whole.astype(half).reshape(per, slots, width)
        for i in range(per):
            if g * per + i > 0:
                start(back_copy(g, i))
        if g == 0:
            ret[0] = whole[:slots].astype(half)

    def grads(h, b):
        some = n // 2
        here = slice(h * some, (h + 1) * some)
        rows = slice(h * some * slots, (h + 1) * some * slots)
        cols = slice(b * width, (b + 1) * width)
        both = over(xbuf[b, here, 0].reshape(some * slots, width), dbuf[rows, :])
        down = over(hbuf[rows, :], xbuf[b, here, 1].reshape(some * slots, width))
        if h == 0:
            acc_g[cols, :] = both[:, :hidden]
            acc_u[cols, :] = both[:, hidden:]
            acc_d[:, cols] = down
        else:
            acc_g[cols, :] += both[:, :hidden]
            acc_u[cols, :] += both[:, hidden:]
            acc_d[:, cols] += down

    lines = n // 2

    def ring_source(j):
        return lax.rem(me + n - 2 * j, n)

    def ring_send(j, source):
        start(remote(mg.at[source], mg.at[source], mx_sem.at[j], {"sp": me ^ 1}))
        if j < lines - 1:
            start(remote(mg.at[source], mg.at[source], mz_sem.at[j + 1], {"sp": lax.rem(me + 2, n)}))

    def ring(j):
        source = ring_source(j)
        spot = mg.at[source]
        if j > 0:
            remote(spot, spot, mz_sem.at[j], {"sp": me ^ 1}).wait_recv()
        ring_send(j, source)

    pl.semaphore_wait(barrier, n + 1)
    for k in range(1, n):
        start(over_sp(k))
    xbuf[q, 0] = send[0]
    spread(0)

    total = width
    row = lax.broadcasted_iota(jnp.int32, (8, total), 0)

    def forward():
        slow = softplus_of_negative(param_ref[...])
        shift = upright(shift_ref[...])
        for h in range(heads):
            cols = slice(h * head_dim, (h + 1) * head_dim)
            conv = conv_ref[:, cols]
            reset = jax.nn.sigmoid(jnp.dot(conv, wr_ref[h], preferred_element_type=f32))
            inp = jax.nn.sigmoid(jnp.dot(conv, wi_ref[h], preferred_element_type=f32))
            log_decay = -8.0 * reset * slow[:, cols] + shift
            decays = jnp.exp(log_decay)
            norm = jnp.sqrt(-jnp.tanh(log_decay) * (decays * decays + 1.0))
            conv = conv.astype(f32)
            dec[:, cols] = decays
            drive[:, cols] = norm * inp * conv
            fac_o[:, cols] = norm * inp
            fac_i[:, cols] = norm * conv * inp * (1.0 - inp)
            fac_r[:, cols] = (-8.0 * slow[:, cols]) * reset * (1.0 - reset)
            grad[:, cols] = inp * conv * decays * decays / norm

    def forward_scan():
        carry = bs_ref[...]
        for i in range(tokens // 8):
            at = slice(8 * i, 8 * i + 8)
            decay = dec[at, :]
            a = decay
            b = drive[at, :]
            for d in (1, 2, 4):
                b = b + a * jnp.where(row >= d, pltpu.roll(b, d, 0), 0.0)
                a = a * jnp.where(row >= d, pltpu.roll(a, d, 0), 1.0)
            state = a * carry + b
            st[at, :] = state
            prev = jnp.where(row >= 1, pltpu.roll(state, 1, 0), carry)
            fac_r[at, :] = fac_r[at, :] * (decay * prev - grad[at, :])
            carry = state[7:8, :]

    def forward_gate():
        for h in range(heads):
            cols = slice(h * head_dim, (h + 1) * head_dim)
            act, slope = gelu_both(gate_ref[:, cols].astype(f32))
            mg[me, :, cols] = (act * st[:, cols]).astype(half)
            act_b[:, cols] = act
            slope_b[:, cols] = st[:, cols] * slope

    def back_products():
        carry_p = jnp.ones((1, total), f32)
        following = jnp.ones((1, total), f32)
        for i in reversed(range(tokens // 8)):
            at = slice(8 * i, 8 * i + 8)
            decay = dec[at, :]
            a = jnp.where(row < 7, pltpu.roll(decay, 7, 0), following)
            following = decay[0:1, :]
            for d, level in ((1, lev0), (2, lev1), (4, lev2)):
                level[at, :] = jnp.where(row < 8 - d, a, 0.0)
                a = a * jnp.where(row < 8 - d, pltpu.roll(a, 8 - d, 0), 1.0)
            drive[at, :] = a
            p = a * carry_p
            prods[at, :] = p
            carry_p = p[0:1, :]

    fillers = [forward, forward_scan, forward_gate, back_products]
    for fill in fillers[:3]:
        fill()
    late = [fillers[3]]
    for copy in loads:
        copy.wait()
    grad_chunks = [functools.partial(grads, 0, b) for b in range(parts)]
    steps = [functools.partial(ring, j) for j in range(lines)]
    for k in range(1, n + 1):
        if k < n:
            spread(k)
        relay(k - 1)
        if k == 1:
            back_products()
        if k >= per + 1 and (k - 1) % per == 0:
            g = (k - 1) // per - 1
            expert(g)
            if g >= 1:
                join_near(g - 1)
            if g >= 2:
                join_far(g - 2)
        if k > 2 * per + 1 and (k - 1) % per != 0 and grad_chunks:
            grad_chunks.pop(0)()
        if k == n - 1:
            steps.pop(0)()
    last = groups - 1
    expert(last)
    join_near(last - 1)
    steps.pop(0)()
    join_far(last - 2)
    join_near(last)
    while grad_chunks:
        grad_chunks.pop(0)()
    join_far(last - 1)
    grads(1, 0)
    if steps:
        steps.pop(0)()
    join_far(last)
    for b in range(1, parts):
        grads(1, b)
    g_copies = []
    for i, (src, dst) in enumerate(((acc_g, gg_hbm), (acc_u, gu_hbm), (acc_d, gd_hbm))):
        copy = pltpu.make_async_copy(src, dst, g_sem.at[i])
        copy.start()
        g_copies.append(copy)
    for k in range(1, n):
        back_copy(k // per, k % per).wait_recv()
    summed = jnp.dot(pick_all, ret[...].reshape(n * slots, width), preferred_element_type=f32)
    dcols[...] = (cot_ref[...].astype(f32) + summed).astype(half)

    some = n // parts
    thin = width // some
    quarter = tokens // parts
    owner_q = lax.div(me, some)

    def blk_copy(i, x):
        peer, part = q * some + i, q ^ x
        at = pl.ds(pl.multiple_of(part * quarter, quarter), quarter)
        return pltpu.make_async_remote_copy(
            src_ref=bsend.at[i, at], dst_ref=got.at[me, at], send_sem=send_sem.at[1],
            recv_sem=blk_sem.at[me], device_id={"sp": peer, "tp": part}, device_id_type=MESH,
        )

    mine_at = pl.ds(pl.multiple_of(q * quarter, quarter), quarter)

    def blk_wait(source):
        spot = got.at[source, mine_at]
        remote(spot, spot, blk_sem.at[source], {"tp": far}).wait_recv()

    def dm_copy(owner, i, other, src):
        return remote(src, dmbuf.at[owner], dm_sem.at[i], {"tp": other})

    start(dm_copy(q, 0, far, dcols))
    start(dm_copy(q, 1, near, dcols))
    for i in range(some):
        bsend[i] = dcols[:, i * thin : (i + 1) * thin]
    for i in range(some):
        for x in range(1, parts):
            start(blk_copy(i, x))

        @pl.when(q * some + i != me)
        def _():
            blk_copy(i, 0).start()

        @pl.when(q * some + i == me)
        def _():
            got[me, mine_at] = bsend[i, mine_at]

    while steps:
        steps.pop(0)()
    dmbuf[q] = dcols[...]

    wo_cols = pl.ds(pl.multiple_of(q * width, width), width)
    grad[...] = against(dcols[...], wo[:, wo_cols])
    dm_copy(far, 0, far, dcols).wait_recv()
    start(dm_copy(far, 2, near, dmbuf.at[far]))
    dm_copy(near, 1, near, dcols).wait_recv()
    dm_copy(near ^ 2, 2, near, dcols).wait_recv()
    for shift_by in (1, 2, 3):
        other = q ^ shift_by
        at = pl.ds(pl.multiple_of(other * width, width), width)
        grad[...] += against(dmbuf[other], wo[:, at])
    for off in range(1, n):
        blk_wait(lax.rem(me + off, n))

    @pl.when(q != owner_q)
    def _():
        blk_wait(me)

    def got_copy(part, i, other):
        at = pl.ds(pl.multiple_of(part * quarter, quarter), quarter)
        spot = got.at[:, at]
        return remote(spot, spot, got_sem.at[i], {"tp": other})

    start(got_copy(q, 0, far))
    start(got_copy(q, 1, near))

    carry = jnp.zeros((1, total), f32)
    for i in reversed(range(tokens // 8)):
        at = slice(8 * i, 8 * i + 8)
        b = grad[at, :]
        gate_out_ref[at, :] = (b * slope_b[at, :]).astype(half)
        b = b * act_b[at, :]
        b = b + lev0[at, :] * pltpu.roll(b, 7, 0)
        b = b + lev1[at, :] * pltpu.roll(b, 6, 0)
        b = b + lev2[at, :] * pltpu.roll(b, 4, 0)
        g = drive[at, :] * carry + b
        grad[at, :] = g
        carry = g[0:1, :]
    first = dec[0:1, :]
    mine_pair[0:1, :] = prods[0:1, :] * first
    mine_pair[1:2, :] = carry * first
    mine_pair[2:8, :] = jnp.zeros((6, total), f32)
    pairs[me] = jnp.zeros((8, total), f32)

    def pair_to(peer, source):
        return remote(mine_pair, pairs.at[source], pair_sem.at[source], {"sp": peer})

    for off in range(1, n):
        start(pair_to(lax.rem(me + off, n), me))
    got_copy(far, 0, far).wait_recv()
    start(got_copy(far, 2, near))
    for off in range(1, n):
        peer = lax.rem(me + off, n)
        pair_to(peer, peer).wait_recv()
    enter = jnp.zeros((1, total), f32)
    for p in reversed(range(n)):
        pair = pairs[p]
        enter = jnp.where(p > me, pair[1:2, :] + pair[0:1, :] * enter, enter)
    for h in range(heads):
        cols = slice(h * head_dim, (h + 1) * head_dim)
        g = grad[:, cols] + prods[:, cols] * enter[:, cols]
        d_r = (g * fac_r[:, cols]).astype(half)
        d_i = (g * fac_i[:, cols]).astype(half)
        out_ref[:, cols] = (
            g * fac_o[:, cols] + against(d_r, wr_ref[h]) + against(d_i, wi_ref[h])
        ).astype(half)
    for j in range(lines):
        spot = mg.at[ring_source(j) ^ 1]
        remote(spot, spot, mx_sem.at[j], {"sp": me ^ 1}).wait_recv()
    got_copy(near, 1, near).wait_recv()
    got_copy(near ^ 2, 2, near).wait_recv()
    go_ref[...] = over(got[...].reshape(n * tokens, thin), mg[...].reshape(n * tokens, width))
    for copy in g_copies:
        copy.wait()
    for copy in sent:
        copy.wait_send()
    for i in range(some):

        @pl.when(q * some + i != me)
        def _():
            blk_copy(i, 0).wait_send()


VM = pl.BlockSpec(memory_space=pltpu.VMEM)


def run_whole(
    n, parts, slots, mixed, cot, ids, weights, conv, gate, bs, param, shift, wr, wi, wg, wu, wd, wo
):
    tokens, width = mixed.shape
    full, hidden = wg.shape
    groups = 4
    per = n // groups
    block = per * slots
    some = n // parts
    thin = width // some
    half, f32 = jnp.bfloat16, jnp.float32
    anywhere = pl.BlockSpec(memory_space=pl.ANY)
    dma, vm = pltpu.SemaphoreType.DMA, pltpu.VMEM
    shape = jax.ShapeDtypeStruct
    return pl.pallas_call(
        functools.partial(whole_kernel, n, groups),
        out_shape=(
            shape((full, hidden), f32), shape((full, hidden), f32), shape((hidden, full), f32),
            shape((thin, width), f32), shape((tokens, width), half), shape((tokens, width), half),
        ),
        in_specs=[VM] * 11 + [anywhere] * 4,
        out_specs=(anywhere,) * 3 + (VM,) * 3,
        scratch_shapes=[
            vm((full, hidden), half), vm((full, hidden), half), vm((hidden, full), half),
            vm((width, full), half),
            vm((n, 2, slots, width), half),
            vm((parts, n, 2, slots, width), half),
            vm((n * slots, 2 * hidden), half), vm((n * slots, hidden), half),
            vm((groups, parts, block, width), half),
            vm((groups, 2, block, width), half),
            vm((groups, block, width), half),
            vm((groups, block, width), half),
            vm((groups, per, slots, width), half),
            vm((n, slots, width), half),
            vm((tokens, width), half),
            vm((parts, tokens, width), half),
            vm((full, hidden), f32), vm((full, hidden), f32), vm((hidden, full), f32),
        ] + [vm((tokens, width), f32)] * 13 + [
            vm((n, tokens, width), half),
            vm((n, tokens, thin), half),
            vm((some, tokens, thin), half),
            vm((8, width), f32),
            vm((n, 8, width), f32),
            dma((2,)), dma((n,)), dma((n,)), dma((n,)), dma((n,)), dma((groups, 2)),
            dma((groups,)), dma((n,)), dma((3,)), dma((4,)), dma((3,)),
            dma((n // 2,)), dma((n // 2,)), dma((n,)), dma((3,)), dma((n,)),
        ],
        compiler_params=pltpu.CompilerParams(
            collective_id=0, has_side_effects=True, vmem_limit_bytes=63000 * 1024
        ),
        cost_estimate=pl.CostEstimate(flops=8_000_000_000, bytes_accessed=80_000_000, transcendentals=0),
    )(mixed, cot, ids, weights, conv, gate, bs, param, shift, wr, wi, wg, wu, wd, wo)


def body(
    conv_out, gate_in, block_states, decay_param, decay_shift, w_reset, w_input, w_out,
    mixed, d_out, expert_ids, route_weights, w_gate, w_up, w_down,
):
    tok_rows, top_k = expert_ids.shape
    experts = lax.axis_size("sp")
    capacity = 2 * tok_rows * top_k // experts
    slots = -(-capacity // 16) * 16
    grad_gate_e, grad_up_e, grad_down_e, grad_out, grad_in, grad_gate = run_whole(
        experts, lax.axis_size("tp"), slots, mixed, d_out, expert_ids.T, route_weights.T,
        conv_out, gate_in, block_states, decay_param[None, :], decay_shift[None, :],
        w_reset, w_input, w_gate[0], w_up[0], w_down[0], w_out,
    )
    return (grad_gate_e[None], grad_up_e[None], grad_down_e[None], grad_out, grad_in, grad_gate)


def solution(mesh):
    placed = (
        P("sp", "tp"),
        P("sp", "tp"),
        P("sp", "tp"),
        P("tp"),
        P("sp"),
        P("tp", None, None),
        P("tp", None, None),
        P("tp", None),
        P("sp", "tp"),
        P("sp", "tp"),
        P("sp", None),
        P("sp", None),
        P("sp", None, "tp"),
        P("sp", None, "tp"),
        P("sp", "tp", None),
    )
    return jax.shard_map(
        body,
        mesh=mesh,
        in_specs=placed,
        out_specs=(
            P("sp", None, "tp"),
            P("sp", None, "tp"),
            P("sp", "tp", None),
            P("sp", "tp"),
            P("sp", "tp"),
            P("sp", "tp"),
        ),
        check_vma=False,
    )
```

```python
import functools
import jax
import jax.numpy as jnp
from jax import lax
from jax.experimental import pallas as pl
from jax.experimental.pallas import tpu as pltpu
from jax.sharding import PartitionSpec as P

MESH = pl.DeviceIdType.MESH
GELU_C = 0.7978845608028654
GELU_K = 0.044715


def gelu_both(x):
    inner = jnp.tanh(GELU_C * (x + GELU_K * x * x * x))
    act = 0.5 * x * (1.0 + inner)
    slope = 0.5 * (1.0 + inner) + 0.5 * x * (1.0 - inner * inner) * (
        GELU_C * (1.0 + 3.0 * GELU_K * x * x)
    )
    return act, slope


def softplus_of_negative(x):
    small = jnp.exp(-jnp.abs(x))
    ratio = small / (2.0 + small)
    square = ratio * ratio
    series = jnp.zeros_like(x)
    for odd in range(17, 0, -2):
        series = series * square + 1.0 / odd
    return jnp.maximum(-x, 0.0) + 2.0 * ratio * series


def whole_kernel(
    n, groups,
    mixed_ref, cot_ref, ids_ref, wts_ref,
    conv_ref, gate_ref, bs_ref, param_ref, shift_ref, wr_ref, wi_ref,
    wg_hbm, wu_hbm, wd_hbm, wo_hbm,
    gg_hbm, gu_hbm, gd_hbm, go_ref, out_ref, gate_out_ref,
    wg, wu, wd, wo, info, tok, send, xbuf, dbuf, hbuf, pbuf, nbuf, sbuf, fbuf, rbuf, ret, dcols, dmbuf,
    acc_g, acc_u, acc_d, dec, drive, st, act_b, slope_b, fac_r, fac_i, fac_o, prods, lev0, lev1, lev2, grad,
    mg, got, bsend, mine_pair, pairs,
    send_sem, tok_send, credit, tok_sem, info_sem, x_sem, y_sem, own_sem, fwd_sem, near_sem, far_sem, ret_sem, dm_sem, w_sem, g_sem,
    mz_sem, mx_sem, blk_sem, got_sem, pair_sem,
):
    me, q = lax.axis_index("sp"), lax.axis_index("tp")
    near, far = q ^ 1, q ^ 2
    barrier = pltpu.get_barrier_semaphore()
    for off in range(1, n):
        pl.semaphore_signal(
            barrier, inc=1, device_id={"sp": lax.rem(me + off, n)}, device_id_type=MESH
        )
    for other in (near, far):
        pl.semaphore_signal(barrier, inc=1, device_id={"tp": other}, device_id_type=MESH)
    loads = [
        pltpu.make_async_copy(src, dst, w_sem.at[i])
        for i, (src, dst) in enumerate(((wg_hbm, wg), (wu_hbm, wu), (wd_hbm, wd), (wo_hbm, wo)))
    ]
    for copy in loads:
        copy.start()
    tokens, width = mixed_ref.shape
    top = ids_ref.shape[0]
    slots = send.shape[2]
    hidden = wg.shape[1]
    parts = xbuf.shape[0]
    per = n // groups
    block = per * slots
    heads, head_dim = wr_ref.shape[0], wr_ref.shape[1]
    f32, half = jnp.float32, jnp.bfloat16

    eye = lax.broadcasted_iota(jnp.int32, (tokens, tokens), 0) == (
        lax.broadcasted_iota(jnp.int32, (tokens, tokens), 1)
    )

    def upright(row):
        return jnp.sum(jnp.where(eye, row, jnp.zeros_like(row)), axis=1, keepdims=True)

    for j in range(top):
        info[0, j : j + 1, :] = ids_ref[j : j + 1, :].astype(f32)
        info[0, top + j : top + j + 1, :] = wts_ref[j : j + 1, :]
    info[0, 2 * top :, :] = jnp.zeros((info.shape[1] - 2 * top, tokens), f32)

    def over(left, right):
        return lax.dot_general(left, right, (((0,), (0,)), ((), ())), preferred_element_type=f32)

    def against(left, right):
        return lax.dot_general(left, right, (((1,), (1,)), ((), ())), preferred_element_type=f32)

    sent = []

    def remote(src, dst, recv, where):
        return pltpu.make_async_remote_copy(
            src_ref=src, dst_ref=dst, send_sem=send_sem.at[0], recv_sem=recv,
            device_id=where, device_id_type=MESH,
        )

    def start(copy):
        copy.start()
        sent.append(copy)

    lines, held = n // 2, tok.shape[0]
    following_line = lax.rem(me + 2, n)

    def ring_copy(j, i):
        source = (mixed_ref, cot_ref)[i] if j == 0 else tok.at[j % held, i]
        return pltpu.make_async_remote_copy(
            src_ref=source, dst_ref=tok.at[(j + 1) % held, i], send_sem=tok_send.at[j, i],
            recv_sem=tok_sem.at[j + 1, i], device_id={"sp": following_line}, device_id_type=MESH,
        )

    def ring_start(j):
        if j + 1 > held:
            pl.semaphore_wait(credit, 1)
        for i in range(2):
            ring_copy(j, i).start()

    def ring_free(j):
        for i in range(2):
            ring_copy(j, i).wait_send()
        if 1 <= j and j + held < lines:
            pl.semaphore_signal(
                credit, inc=1, device_id={"sp": lax.rem(me + n - 2, n)}, device_id_type=MESH
            )

    def info_copy(j):
        return remote(info.at[0], info.at[j], info_sem.at[j], {"sp": lax.rem(me + 2 * j, n)})

    def cross_copy(j):
        return remote(send.at[j], xbuf.at[q, 2 * j + 1], x_sem.at[j], {"sp": me ^ 1})

    slot = lax.broadcasted_iota(jnp.int32, (slots, tokens), 0)
    before = lax.broadcasted_iota(jnp.int32, (tokens, tokens), 0) < (
        lax.broadcasted_iota(jnp.int32, (tokens, tokens), 1)
    )

    def arrive(j):
        if j > 0:
            for i in range(2):
                ring_copy(j - 1, i).wait_recv()
            if j < lines - 1:
                ring_start(j)
            ring_free(j - 1)
            info_copy(j).wait_recv()
        rows = mixed_ref[...] if j == 0 else tok[j % held, 0]
        cots = cot_ref[...] if j == 0 else tok[j % held, 1]
        ids = [info[j, i : i + 1, :].astype(jnp.int32) for i in range(top)]
        which = lax.broadcasted_iota(jnp.int32, (8, tokens), 0)
        wanted = jnp.where(which == 0, me, me ^ 1)
        hit = jnp.zeros((8, tokens), f32)
        weight = jnp.zeros((8, tokens), f32)
        for i in range(top):
            same = ids[i] == wanted
            hit = jnp.where(same, 1.0, hit)
            weight = jnp.where(same, info[j, top + i : top + i + 1, :], weight)
        order = jnp.dot(
            hit.astype(half), jnp.where(before, 1.0, 0.0).astype(half), preferred_element_type=f32
        )
        order = jnp.where(hit > 0.5, order, -1.0).astype(jnp.int32)
        for side in (1, 0):
            chosen = slot == order[side : side + 1, :]
            pick = jnp.where(chosen, 1.0, 0.0).astype(half)
            scale = jnp.sum(
                jnp.where(chosen, weight[side : side + 1, :], 0.0), axis=1, keepdims=True
            )
            x = jnp.dot(pick, rows, preferred_element_type=f32).astype(half)
            c = (scale * jnp.dot(pick, cots, preferred_element_type=f32)).astype(half)
            if side == 1:
                send[j, 0] = x
                send[j, 1] = c
                start(cross_copy(j))
            else:
                xbuf[q, 2 * j, 0] = x
                xbuf[q, 2 * j, 1] = c
                spread(2 * j)

    def crossed(j):
        cross_copy(j).wait_recv()
        spread(2 * j + 1)

    def over_tp(owner, k, other, sems):
        spot = xbuf.at[owner, k]
        return remote(spot, spot, sems.at[k], {"tp": other})

    def spread(k):
        start(over_tp(q, k, far, y_sem))
        start(over_tp(q, k, near, own_sem))

    def relay(k):
        over_tp(far, k, far, y_sem).wait_recv()
        start(over_tp(far, k, near, fwd_sem))

    def near_copy(g, i):
        return remote(
            pbuf.at[g, near if i == 0 else far ^ 1], nbuf.at[g, i], near_sem.at[g, i], {"tp": near}
        )

    def expert(g):
        for k in range(g * per, (g + 1) * per):
            over_tp(near, k, near, own_sem).wait_recv()
            over_tp(near ^ 2, k, near, fwd_sem).wait_recv()
        here = slice(g * per, (g + 1) * per)
        up_pre = jnp.zeros((block, hidden), f32)
        linear = jnp.zeros((block, hidden), f32)
        d_hidden = jnp.zeros((block, hidden), f32)
        for b in range(parts):
            cols = slice(b * width, (b + 1) * width)
            x = xbuf[b, here, 0].reshape(block, width)
            c = xbuf[b, here, 1].reshape(block, width)
            up_pre += jnp.dot(x, wg[cols, :], preferred_element_type=f32)
            linear += jnp.dot(x, wu[cols, :], preferred_element_type=f32)
            d_hidden += against(c, wd[:, cols])
        sig = jax.nn.sigmoid(up_pre)
        silu = up_pre * sig
        rows = slice(g * block, (g + 1) * block)
        hbuf[rows, :] = (silu * linear).astype(half)
        d_linear = (d_hidden * silu).astype(half)
        d_up = (d_hidden * linear * sig * (1.0 + up_pre * (1.0 - sig))).astype(half)
        dbuf[rows, :hidden] = d_up
        dbuf[rows, hidden:] = d_linear
        for b in range(parts):
            cols = slice(b * width, (b + 1) * width)
            pbuf[g, b] = (against(d_up, wg[cols, :]) + against(d_linear, wu[cols, :])).astype(half)
        for i in range(2):
            start(near_copy(g, 1 - i))

    def far_copy(g):
        return remote(sbuf.at[g], fbuf.at[g], far_sem.at[g], {"tp": far})

    def join_near(g):
        near_copy(g, 1).wait_recv()
        sbuf[g] = (pbuf[g, far].astype(f32) + nbuf[g, 1].astype(f32)).astype(half)
        start(far_copy(g))

    def back_copy(g, i):
        k = g * per + i
        return remote(
            rbuf.at[g, i], ret.at[k], ret_sem.at[k],
            {"sp": lax.rem(me + n - 2 * (k // 2), n) ^ (k % 2)},
        )

    def join_far(g):
        near_copy(g, 0).wait_recv()
        far_copy(g).wait_recv()
        whole = pbuf[g, q].astype(f32) + nbuf[g, 0].astype(f32) + fbuf[g].astype(f32)
        rbuf[g] = whole.astype(half).reshape(per, slots, width)
        for i in range(per):
            if g * per + i > 0:
                start(back_copy(g, i))
        if g == 0:
            ret[0] = whole[:slots].astype(half)

    def grads(h, b):
        some = n // 2
        here = slice(h * some, (h + 1) * some)
        rows = slice(h * some * slots, (h + 1) * some * slots)
        cols = slice(b * width, (b + 1) * width)
        both = over(xbuf[b, here, 0].reshape(some * slots, width), dbuf[rows, :])
        down = over(hbuf[rows, :], xbuf[b, here, 1].reshape(some * slots, width))
        if h == 0:
            acc_g[cols, :] = both[:, :hidden]
            acc_u[cols, :] = both[:, hidden:]
            acc_d[:, cols] = down
        else:
            acc_g[cols, :] += both[:, :hidden]
            acc_u[cols, :] += both[:, hidden:]
            acc_d[:, cols] += down

    def ring_source(j):
        return lax.rem(me + n - 2 * j, n)

    def ring_send(j, source):
        start(remote(mg.at[source], mg.at[source], mx_sem.at[j], {"sp": me ^ 1}))
        if j < lines - 1:
            start(remote(mg.at[source], mg.at[source], mz_sem.at[j + 1], {"sp": lax.rem(me + 2, n)}))

    def ring(j):
        source = ring_source(j)
        spot = mg.at[source]
        if j > 0:
            remote(spot, spot, mz_sem.at[j], {"sp": me ^ 1}).wait_recv()
        ring_send(j, source)

    pl.semaphore_wait(barrier, n + 1)
    ring_start(0)
    for j in range(1, lines):
        start(info_copy(j))
    arrive(0)

    total = width
    row = lax.broadcasted_iota(jnp.int32, (8, total), 0)

    def forward():
        slow = softplus_of_negative(param_ref[...])
        shift = upright(shift_ref[...])
        for h in range(heads):
            cols = slice(h * head_dim, (h + 1) * head_dim)
            conv = conv_ref[:, cols]
            reset = jax.nn.sigmoid(jnp.dot(conv, wr_ref[h], preferred_element_type=f32))
            inp = jax.nn.sigmoid(jnp.dot(conv, wi_ref[h], preferred_element_type=f32))
            log_decay = -8.0 * reset * slow[:, cols] + shift
            decays = jnp.exp(log_decay)
            norm = jnp.sqrt(-jnp.tanh(log_decay) * (decays * decays + 1.0))
            conv = conv.astype(f32)
            dec[:, cols] = decays
            drive[:, cols] = norm * inp * conv
            fac_o[:, cols] = norm * inp
            fac_i[:, cols] = norm * conv * inp * (1.0 - inp)
            fac_r[:, cols] = (-8.0 * slow[:, cols]) * reset * (1.0 - reset)
            grad[:, cols] = inp * conv * decays * decays / norm

    def forward_scan():
        carry = bs_ref[...]
        for i in range(tokens // 8):
            at = slice(8 * i, 8 * i + 8)
            decay = dec[at, :]
            a = decay
            b = drive[at, :]
            for d in (1, 2, 4):
                b = b + a * jnp.where(row >= d, pltpu.roll(b, d, 0), 0.0)
                a = a * jnp.where(row >= d, pltpu.roll(a, d, 0), 1.0)
            state = a * carry + b
            st[at, :] = state
            prev = jnp.where(row >= 1, pltpu.roll(state, 1, 0), carry)
            fac_r[at, :] = fac_r[at, :] * (decay * prev - grad[at, :])
            carry = state[7:8, :]

    def forward_gate():
        for h in range(heads):
            cols = slice(h * head_dim, (h + 1) * head_dim)
            act, slope = gelu_both(gate_ref[:, cols].astype(f32))
            mg[me, :, cols] = (act * st[:, cols]).astype(half)
            act_b[:, cols] = act
            slope_b[:, cols] = st[:, cols] * slope

    def back_products():
        carry_p = jnp.ones((1, total), f32)
        following = jnp.ones((1, total), f32)
        for i in reversed(range(tokens // 8)):
            at = slice(8 * i, 8 * i + 8)
            decay = dec[at, :]
            a = jnp.where(row < 7, pltpu.roll(decay, 7, 0), following)
            following = decay[0:1, :]
            for d, level in ((1, lev0), (2, lev1), (4, lev2)):
                level[at, :] = jnp.where(row < 8 - d, a, 0.0)
                a = a * jnp.where(row < 8 - d, pltpu.roll(a, 8 - d, 0), 1.0)
            drive[at, :] = a
            p = a * carry_p
            prods[at, :] = p
            carry_p = p[0:1, :]

    forward()
    forward_scan()
    crossed(0)
    relay(0)
    forward_gate()
    back_products()
    for copy in loads:
        copy.wait()
    grad_chunks = [functools.partial(grads, 0, b) for b in range(parts)]
    steps = [functools.partial(ring, j) for j in range(lines)]
    line_group = per // 2
    for j in range(1, lines):
        arrive(j)
        relay(2 * j - 1)
        if j == lines - 1:
            steps.pop(0)()
        g = j // line_group
        if j % line_group == 0:
            expert(g - 1)
            if g >= 2:
                join_near(g - 2)
            if g >= 3:
                join_far(g - 3)
        crossed(j)
        relay(2 * j)
        if g > groups // 2 and grad_chunks:
            grad_chunks.pop(0)()
    last = groups - 1
    join_near(last - 1)
    relay(n - 1)
    steps.pop(0)()
    expert(last)
    join_far(last - 2)
    join_near(last)
    if steps:
        steps.pop(0)()
    while grad_chunks:
        grad_chunks.pop(0)()
    join_far(last - 1)
    grads(1, 0)
    if steps:
        steps.pop(0)()
    join_far(last)
    for b in range(1, parts):
        grads(1, b)
    g_copies = []
    for i, (src, dst) in enumerate(((acc_g, gg_hbm), (acc_u, gu_hbm), (acc_d, gd_hbm))):
        copy = pltpu.make_async_copy(src, dst, g_sem.at[i])
        copy.start()
        g_copies.append(copy)
    lane = lax.broadcasted_iota(jnp.int32, (tokens, 128), 1)
    away = []
    for j in range(top):
        named = upright(info[0, j : j + 1, :]).astype(jnp.int32)
        gap = lax.shift_right_logical(named, 1) - lax.div(me, 2)
        gap = jnp.where(gap < 0, gap + lines, gap)
        away.append(2 * gap + ((named ^ me) & 1))
    member = jnp.zeros((tokens, 128), f32)
    for j in range(top):
        member = jnp.where(away[j] == lane, 1.0, member)
    earlier = lax.broadcasted_iota(jnp.int32, (tokens, tokens), 1) < (
        lax.broadcasted_iota(jnp.int32, (tokens, tokens), 0)
    )
    rank = jnp.dot(
        jnp.where(earlier, 1.0, 0.0).astype(half), member.astype(half), preferred_element_type=f32
    )
    place = lax.broadcasted_iota(jnp.int32, (tokens, n * slots), 1)
    pick_all = jnp.zeros((tokens, n * slots), f32)
    for j in range(top):
        mine = jnp.sum(jnp.where(away[j] == lane, rank, 0.0), axis=1, keepdims=True)
        pick_all = jnp.where(place == away[j] * slots + mine.astype(jnp.int32), 1.0, pick_all)
    pick_all = pick_all.astype(half)
    for k in range(1, n):
        back_copy(k // per, k % per).wait_recv()
    summed = jnp.dot(pick_all, ret[...].reshape(n * slots, width), preferred_element_type=f32)
    dcols[...] = (cot_ref[...].astype(f32) + summed).astype(half)

    some = n // parts
    thin = width // some
    quarter = tokens // parts
    owner_q = lax.div(me, some)

    def blk_copy(i, x):
        peer, part = q * some + i, q ^ x
        at = pl.ds(pl.multiple_of(part * quarter, quarter), quarter)
        return pltpu.make_async_remote_copy(
            src_ref=bsend.at[i, at], dst_ref=got.at[me, at], send_sem=send_sem.at[1],
            recv_sem=blk_sem.at[me], device_id={"sp": peer, "tp": part}, device_id_type=MESH,
        )

    mine_at = pl.ds(pl.multiple_of(q * quarter, quarter), quarter)

    def blk_wait(source):
        spot = got.at[source, mine_at]
        remote(spot, spot, blk_sem.at[source], {"tp": far}).wait_recv()

    def dm_copy(owner, i, other, src):
        return remote(src, dmbuf.at[owner], dm_sem.at[i], {"tp": other})

    start(dm_copy(q, 0, far, dcols))
    start(dm_copy(q, 1, near, dcols))
    for i in range(some):
        bsend[i] = dcols[:, i * thin : (i + 1) * thin]
    for i in range(some):
        for x in range(1, parts):
            start(blk_copy(i, x))

        @pl.when(q * some + i != me)
        def _():
            blk_copy(i, 0).start()

        @pl.when(q * some + i == me)
        def _():
            got[me, mine_at] = bsend[i, mine_at]

    while steps:
        steps.pop(0)()
    dmbuf[q] = dcols[...]

    wo_cols = pl.ds(pl.multiple_of(q * width, width), width)
    grad[...] = against(dcols[...], wo[:, wo_cols])
    dm_copy(far, 0, far, dcols).wait_recv()
    start(dm_copy(far, 2, near, dmbuf.at[far]))
    dm_copy(near, 1, near, dcols).wait_recv()
    dm_copy(near ^ 2, 2, near, dcols).wait_recv()
    for shift_by in (1, 2, 3):
        other = q ^ shift_by
        at = pl.ds(pl.multiple_of(other * width, width), width)
        grad[...] += against(dmbuf[other], wo[:, at])
    for off in range(1, n):
        blk_wait(lax.rem(me + off, n))

    @pl.when(q != owner_q)
    def _():
        blk_wait(me)

    def got_copy(part, i, other):
        at = pl.ds(pl.multiple_of(part * quarter, quarter), quarter)
        spot = got.at[:, at]
        return remote(spot, spot, got_sem.at[i], {"tp": other})

    start(got_copy(q, 0, far))
    start(got_copy(q, 1, near))

    carry = jnp.zeros((1, total), f32)
    for i in reversed(range(tokens // 8)):
        at = slice(8 * i, 8 * i + 8)
        b = grad[at, :]
        gate_out_ref[at, :] = (b * slope_b[at, :]).astype(half)
        b = b * act_b[at, :]
        b = b + lev0[at, :] * pltpu.roll(b, 7, 0)
        b = b + lev1[at, :] * pltpu.roll(b, 6, 0)
        b = b + lev2[at, :] * pltpu.roll(b, 4, 0)
        g = drive[at, :] * carry + b
        grad[at, :] = g
        carry = g[0:1, :]
    first = dec[0:1, :]
    mine_pair[0:1, :] = prods[0:1, :] * first
    mine_pair[1:2, :] = carry * first
    mine_pair[2:8, :] = jnp.zeros((6, total), f32)
    pairs[me] = jnp.zeros((8, total), f32)

    def pair_to(peer, source):
        return remote(mine_pair, pairs.at[source], pair_sem.at[source], {"sp": peer})

    for off in range(1, n):
        start(pair_to(lax.rem(me + off, n), me))
    got_copy(far, 0, far).wait_recv()
    start(got_copy(far, 2, near))
    for off in range(1, n):
        peer = lax.rem(me + off, n)
        pair_to(peer, peer).wait_recv()
    enter = jnp.zeros((1, total), f32)
    for p in reversed(range(n)):
        pair = pairs[p]
        enter = jnp.where(p > me, pair[1:2, :] + pair[0:1, :] * enter, enter)
    for h in range(heads):
        cols = slice(h * head_dim, (h + 1) * head_dim)
        g = grad[:, cols] + prods[:, cols] * enter[:, cols]
        d_r = (g * fac_r[:, cols]).astype(half)
        d_i = (g * fac_i[:, cols]).astype(half)
        out_ref[:, cols] = (
            g * fac_o[:, cols] + against(d_r, wr_ref[h]) + against(d_i, wi_ref[h])
        ).astype(half)
    for j in range(lines):
        spot = mg.at[ring_source(j) ^ 1]
        remote(spot, spot, mx_sem.at[j], {"sp": me ^ 1}).wait_recv()
    got_copy(near, 1, near).wait_recv()
    got_copy(near ^ 2, 2, near).wait_recv()
    go_ref[...] = over(got[...].reshape(n * tokens, thin), mg[...].reshape(n * tokens, width))
    for copy in g_copies:
        copy.wait()
    for copy in sent:
        copy.wait_send()
    for i in range(some):

        @pl.when(q * some + i != me)
        def _():
            blk_copy(i, 0).wait_send()


VM = pl.BlockSpec(memory_space=pltpu.VMEM)


def run_whole(
    n, parts, slots, mixed, cot, ids, weights, conv, gate, bs, param, shift, wr, wi, wg, wu, wd, wo
):
    tokens, width = mixed.shape
    full, hidden = wg.shape
    groups = 4
    per = n // groups
    block = per * slots
    some = n // parts
    thin = width // some
    half, f32 = jnp.bfloat16, jnp.float32
    anywhere = pl.BlockSpec(memory_space=pl.ANY)
    dma, vm = pltpu.SemaphoreType.DMA, pltpu.VMEM
    shape = jax.ShapeDtypeStruct
    return pl.pallas_call(
        functools.partial(whole_kernel, n, groups),
        out_shape=(
            shape((full, hidden), f32), shape((full, hidden), f32), shape((hidden, full), f32),
            shape((thin, width), f32), shape((tokens, width), half), shape((tokens, width), half),
        ),
        in_specs=[VM] * 11 + [anywhere] * 4,
        out_specs=(anywhere,) * 3 + (VM,) * 3,
        scratch_shapes=[
            vm((full, hidden), half), vm((full, hidden), half), vm((hidden, full), half),
            vm((width, full), half),
            vm((n // 2, 8, tokens), f32),
            vm((min(n // 2, 8), 2, tokens, width), half),
            vm((n // 2, 2, slots, width), half),
            vm((parts, n, 2, slots, width), half),
            vm((n * slots, 2 * hidden), half), vm((n * slots, hidden), half),
            vm((groups, parts, block, width), half),
            vm((groups, 2, block, width), half),
            vm((groups, block, width), half),
            vm((groups, block, width), half),
            vm((groups, per, slots, width), half),
            vm((n, slots, width), half),
            vm((tokens, width), half),
            vm((parts, tokens, width), half),
            vm((full, hidden), f32), vm((full, hidden), f32), vm((hidden, full), f32),
        ] + [vm((tokens, width), f32)] * 13 + [
            vm((n, tokens, width), half),
            vm((n, tokens, thin), half),
            vm((some, tokens, thin), half),
            vm((8, width), f32),
            vm((n, 8, width), f32),
            dma((2,)), dma((n // 2, 2)), pltpu.SemaphoreType.REGULAR, dma((n // 2, 2)), dma((n // 2,)), dma((n // 2,)), dma((n,)), dma((n,)), dma((n,)),
            dma((groups, 2)),
            dma((groups,)), dma((n,)), dma((3,)), dma((4,)), dma((3,)),
            dma((n // 2,)), dma((n // 2,)), dma((n,)), dma((3,)), dma((n,)),
        ],
        compiler_params=pltpu.CompilerParams(
            collective_id=0, has_side_effects=True, vmem_limit_bytes=63000 * 1024
        ),
        cost_estimate=pl.CostEstimate(flops=8_000_000_000, bytes_accessed=80_000_000, transcendentals=0),
    )(mixed, cot, ids, weights, conv, gate, bs, param, shift, wr, wi, wg, wu, wd, wo)


def body(
    conv_out, gate_in, block_states, decay_param, decay_shift, w_reset, w_input, w_out,
    mixed, d_out, expert_ids, route_weights, w_gate, w_up, w_down,
):
    tok_rows, top_k = expert_ids.shape
    experts = lax.axis_size("sp")
    capacity = 2 * tok_rows * top_k // experts
    slots = -(-capacity // 16) * 16
    grad_gate_e, grad_up_e, grad_down_e, grad_out, grad_in, grad_gate = run_whole(
        experts, lax.axis_size("tp"), slots, mixed, d_out, expert_ids.T, route_weights.T,
        conv_out, gate_in, block_states, decay_param[None, :], decay_shift[None, :],
        w_reset, w_input, w_gate[0], w_up[0], w_down[0], w_out,
    )
    return (grad_gate_e[None], grad_up_e[None], grad_down_e[None], grad_out, grad_in, grad_gate)


def solution(mesh):
    placed = (
        P("sp", "tp"),
        P("sp", "tp"),
        P("sp", "tp"),
        P("tp"),
        P("sp"),
        P("tp", None, None),
        P("tp", None, None),
        P("tp", None),
        P("sp", "tp"),
        P("sp", "tp"),
        P("sp", None),
        P("sp", None),
        P("sp", None, "tp"),
        P("sp", None, "tp"),
        P("sp", "tp", None),
    )
    return jax.shard_map(
        body,
        mesh=mesh,
        in_specs=placed,
        out_specs=(
            P("sp", None, "tp"),
            P("sp", None, "tp"),
            P("sp", "tp", None),
            P("sp", "tp"),
            P("sp", "tp"),
            P("sp", "tp"),
        ),
        check_vma=False,
    )
```

```python
import functools
import jax
import jax.numpy as jnp
from jax import lax
from jax.experimental import pallas as pl
from jax.experimental.pallas import tpu as pltpu
from jax.sharding import PartitionSpec as P

MESH = pl.DeviceIdType.MESH
GELU_C = 0.7978845608028654
GELU_K = 0.044715


def gelu_both(x):
    inner = jnp.tanh(GELU_C * (x + GELU_K * x * x * x))
    act = 0.5 * x * (1.0 + inner)
    slope = 0.5 * (1.0 + inner) + 0.5 * x * (1.0 - inner * inner) * (
        GELU_C * (1.0 + 3.0 * GELU_K * x * x)
    )
    return act, slope


def softplus_of_negative(x):
    small = jnp.exp(-jnp.abs(x))
    ratio = small / (2.0 + small)
    square = ratio * ratio
    series = jnp.zeros_like(x)
    for odd in range(17, 0, -2):
        series = series * square + 1.0 / odd
    return jnp.maximum(-x, 0.0) + 2.0 * ratio * series


def whole_kernel(
    n, groups,
    mixed_hbm, cot_hbm, ids_hbm, wts_hbm,
    conv_hbm, gate_hbm, bs_hbm, param_hbm, shift_hbm, wr_hbm, wi_hbm,
    wg_hbm, wu_hbm, wd_hbm, wo_hbm,
    acc_g, acc_u, acc_d, go_ref, out_ref, gate_out_ref,
    mixed_ref, cot_ref, ids_ref, wts_ref,
    conv_ref, gate_ref, bs_ref, param_ref, shift_ref, wr_ref, wi_ref,
    wg, wu, wd, wo, info, tok, send, xbuf, dbuf, hbuf, pbuf, nbuf, sbuf, fbuf, rbuf, ret, dcols, dmbuf,
    dec, drive, st, act_b, slope_b, fac_r, fac_i, fac_o, prods, lev0, lev1, lev2, grad,
    mg, got, bsend, mine_pair, pairs,
    send_sem, tok_send, credit, tok_sem, info_sem, x_sem, y_sem, own_sem, fwd_sem, near_sem, far_sem, ret_sem, dm_sem, w_sem,
    mz_sem, mx_sem, blk_sem, got_sem, pair_sem,
):
    me, q = lax.axis_index("sp"), lax.axis_index("tp")
    near, far = q ^ 1, q ^ 2
    barrier = pltpu.get_barrier_semaphore()
    for off in range(1, n):
        pl.semaphore_signal(
            barrier, inc=1, device_id={"sp": lax.rem(me + off, n)}, device_id_type=MESH
        )
    for other in (near, far):
        pl.semaphore_signal(barrier, inc=1, device_id={"tp": other}, device_id_type=MESH)
    pairs_in = (
        (ids_hbm, ids_ref), (wts_hbm, wts_ref), (mixed_hbm, mixed_ref), (cot_hbm, cot_ref),
        (conv_hbm, conv_ref), (gate_hbm, gate_ref), (bs_hbm, bs_ref), (param_hbm, param_ref),
        (shift_hbm, shift_ref), (wr_hbm, wr_ref), (wi_hbm, wi_ref),
        (wg_hbm, wg), (wu_hbm, wu), (wd_hbm, wd), (wo_hbm, wo),
    )
    loads = [
        pltpu.make_async_copy(src, dst, w_sem.at[i]) for i, (src, dst) in enumerate(pairs_in)
    ]
    for copy in loads:
        copy.start()
    tokens, width = mixed_ref.shape
    top = ids_ref.shape[0]
    slots = send.shape[2]
    hidden = wg.shape[1]
    parts = xbuf.shape[0]
    per = n // groups
    block = per * slots
    heads, head_dim = wr_ref.shape[0], wr_ref.shape[1]
    f32, half = jnp.float32, jnp.bfloat16

    eye = lax.broadcasted_iota(jnp.int32, (tokens, tokens), 0) == (
        lax.broadcasted_iota(jnp.int32, (tokens, tokens), 1)
    )

    def upright(row):
        return jnp.sum(jnp.where(eye, row, jnp.zeros_like(row)), axis=1, keepdims=True)

    for copy in loads[:2]:
        copy.wait()
    for j in range(top):
        info[0, j : j + 1, :] = ids_ref[j : j + 1, :].astype(f32)
        info[0, top + j : top + j + 1, :] = wts_ref[j : j + 1, :]
    info[0, 2 * top :, :] = jnp.zeros((info.shape[1] - 2 * top, tokens), f32)

    def over(left, right):
        return lax.dot_general(left, right, (((0,), (0,)), ((), ())), preferred_element_type=f32)

    def against(left, right):
        return lax.dot_general(left, right, (((1,), (1,)), ((), ())), preferred_element_type=f32)

    sent = []

    def remote(src, dst, recv, where):
        return pltpu.make_async_remote_copy(
            src_ref=src, dst_ref=dst, send_sem=send_sem.at[0], recv_sem=recv,
            device_id=where, device_id_type=MESH,
        )

    def start(copy):
        copy.start()
        sent.append(copy)

    lines, held = n // 2, tok.shape[0]
    following_line = lax.rem(me + 2, n)

    def ring_copy(j, i):
        source = (mixed_hbm, cot_hbm)[i] if j == 0 else tok.at[j % held, i]
        return pltpu.make_async_remote_copy(
            src_ref=source, dst_ref=tok.at[(j + 1) % held, i], send_sem=tok_send.at[j, i],
            recv_sem=tok_sem.at[j + 1, i], device_id={"sp": following_line}, device_id_type=MESH,
        )

    def ring_start(j):
        if j + 1 > held:
            pl.semaphore_wait(credit, 1)
        for i in range(2):
            ring_copy(j, i).start()

    def ring_free(j):
        for i in range(2):
            ring_copy(j, i).wait_send()
        if 1 <= j and j + held < lines:
            pl.semaphore_signal(
                credit, inc=1, device_id={"sp": lax.rem(me + n - 2, n)}, device_id_type=MESH
            )

    def info_copy(j):
        return remote(info.at[0], info.at[j], info_sem.at[j], {"sp": lax.rem(me + 2 * j, n)})

    def cross_copy(j):
        return remote(send.at[j], xbuf.at[q, 2 * j + 1], x_sem.at[j], {"sp": me ^ 1})

    slot = lax.broadcasted_iota(jnp.int32, (slots, tokens), 0)
    before = lax.broadcasted_iota(jnp.int32, (tokens, tokens), 0) < (
        lax.broadcasted_iota(jnp.int32, (tokens, tokens), 1)
    )

    def arrive(j):
        if j > 0:
            for i in range(2):
                ring_copy(j - 1, i).wait_recv()
            if j < lines - 1:
                ring_start(j)
            info_copy(j).wait_recv()
        rows = mixed_ref[...] if j == 0 else tok[j % held, 0]
        cots = cot_ref[...] if j == 0 else tok[j % held, 1]
        ids = [info[j, i : i + 1, :].astype(jnp.int32) for i in range(top)]
        which = lax.broadcasted_iota(jnp.int32, (8, tokens), 0)
        wanted = jnp.where(which == 0, me, me ^ 1)
        hit = jnp.zeros((8, tokens), f32)
        weight = jnp.zeros((8, tokens), f32)
        for i in range(top):
            same = ids[i] == wanted
            hit = jnp.where(same, 1.0, hit)
            weight = jnp.where(same, info[j, top + i : top + i + 1, :], weight)
        order = jnp.dot(
            hit.astype(half), jnp.where(before, 1.0, 0.0).astype(half), preferred_element_type=f32
        )
        order = jnp.where(hit > 0.5, order, -1.0).astype(jnp.int32)
        for side in (1, 0):
            chosen = slot == order[side : side + 1, :]
            pick = jnp.where(chosen, 1.0, 0.0).astype(half)
            scale = jnp.sum(
                jnp.where(chosen, weight[side : side + 1, :], 0.0), axis=1, keepdims=True
            )
            x = jnp.dot(pick, rows, preferred_element_type=f32).astype(half)
            c = (scale * jnp.dot(pick, cots, preferred_element_type=f32)).astype(half)
            if side == 1:
                send[j, 0] = x
                send[j, 1] = c
                start(cross_copy(j))
            else:
                xbuf[q, 2 * j, 0] = x
                xbuf[q, 2 * j, 1] = c
                spread(2 * j)
        if j > 0:
            ring_free(j - 1)

    def crossed(j):
        cross_copy(j).wait_recv()
        spread(2 * j + 1)

    def over_tp(owner, k, other, sems):
        spot = xbuf.at[owner, k]
        return remote(spot, spot, sems.at[k], {"tp": other})

    def spread(k):
        start(over_tp(q, k, far, y_sem))
        start(over_tp(q, k, near, own_sem))

    def relay(k):
        over_tp(far, k, far, y_sem).wait_recv()
        start(over_tp(far, k, near, fwd_sem))

    def near_copy(g, i):
        return remote(
            pbuf.at[g, near if i == 0 else far ^ 1], nbuf.at[g, i], near_sem.at[g, i], {"tp": near}
        )

    def expert(g):
        for k in range(g * per, (g + 1) * per):
            over_tp(near, k, near, own_sem).wait_recv()
            over_tp(near ^ 2, k, near, fwd_sem).wait_recv()
        here = slice(g * per, (g + 1) * per)
        up_pre = jnp.zeros((block, hidden), f32)
        linear = jnp.zeros((block, hidden), f32)
        d_hidden = jnp.zeros((block, hidden), f32)
        for b in range(parts):
            cols = slice(b * width, (b + 1) * width)
            x = xbuf[b, here, 0].reshape(block, width)
            c = xbuf[b, here, 1].reshape(block, width)
            up_pre += jnp.dot(x, wg[cols, :], preferred_element_type=f32)
            linear += jnp.dot(x, wu[cols, :], preferred_element_type=f32)
            d_hidden += against(c, wd[:, cols])
        sig = jax.nn.sigmoid(up_pre)
        silu = up_pre * sig
        rows = slice(g * block, (g + 1) * block)
        hbuf[rows, :] = (silu * linear).astype(half)
        d_linear = (d_hidden * silu).astype(half)
        d_up = (d_hidden * linear * sig * (1.0 + up_pre * (1.0 - sig))).astype(half)
        dbuf[rows, :hidden] = d_up
        dbuf[rows, hidden:] = d_linear
        for b in range(parts):
            cols = slice(b * width, (b + 1) * width)
            pbuf[g, b] = (against(d_up, wg[cols, :]) + against(d_linear, wu[cols, :])).astype(half)
        for i in range(2):
            start(near_copy(g, 1 - i))

    def far_copy(g):
        return remote(sbuf.at[g], fbuf.at[g], far_sem.at[g], {"tp": far})

    def join_near(g):
        near_copy(g, 1).wait_recv()
        sbuf[g] = (pbuf[g, far].astype(f32) + nbuf[g, 1].astype(f32)).astype(half)
        start(far_copy(g))

    def back_copy(g, i):
        k = g * per + i
        return remote(
            rbuf.at[g, i], ret.at[k], ret_sem.at[k],
            {"sp": lax.rem(me + n - 2 * (k // 2), n) ^ (k % 2)},
        )

    def join_far(g):
        near_copy(g, 0).wait_recv()
        far_copy(g).wait_recv()
        whole = pbuf[g, q].astype(f32) + nbuf[g, 0].astype(f32) + fbuf[g].astype(f32)
        rbuf[g] = whole.astype(half).reshape(per, slots, width)
        for i in range(per):
            if g * per + i > 0:
                start(back_copy(g, i))
        if g == 0:
            ret[0] = whole[:slots].astype(half)

    def grads(h, b):
        some = n // 2
        here = slice(h * some, (h + 1) * some)
        rows = slice(h * some * slots, (h + 1) * some * slots)
        cols = slice(b * width, (b + 1) * width)
        both = over(xbuf[b, here, 0].reshape(some * slots, width), dbuf[rows, :])
        down = over(hbuf[rows, :], xbuf[b, here, 1].reshape(some * slots, width))
        if h == 0:
            acc_g[cols, :] = both[:, :hidden]
            acc_u[cols, :] = both[:, hidden:]
            acc_d[:, cols] = down
        else:
            acc_g[cols, :] += both[:, :hidden]
            acc_u[cols, :] += both[:, hidden:]
            acc_d[:, cols] += down

    def ring_source(j):
        return lax.rem(me + n - 2 * j, n)

    def ring_send(j, source):
        start(remote(mg.at[source], mg.at[source], mx_sem.at[j], {"sp": me ^ 1}))
        if j < lines - 1:
            start(remote(mg.at[source], mg.at[source], mz_sem.at[j + 1], {"sp": lax.rem(me + 2, n)}))

    def ring(j):
        source = ring_source(j)
        spot = mg.at[source]
        if j > 0:
            remote(spot, spot, mz_sem.at[j], {"sp": me ^ 1}).wait_recv()
        ring_send(j, source)

    pl.semaphore_wait(barrier, n + 1)
    ring_start(0)
    for j in range(1, lines):
        start(info_copy(j))
    for copy in loads[2:4]:
        copy.wait()
    arrive(0)

    total = width
    row = lax.broadcasted_iota(jnp.int32, (8, total), 0)

    def forward():
        slow = softplus_of_negative(param_ref[...])
        shift = upright(shift_ref[...])
        for h in range(heads):
            cols = slice(h * head_dim, (h + 1) * head_dim)
            conv = conv_ref[:, cols]
            reset = jax.nn.sigmoid(jnp.dot(conv, wr_ref[h], preferred_element_type=f32))
            inp = jax.nn.sigmoid(jnp.dot(conv, wi_ref[h], preferred_element_type=f32))
            log_decay = -8.0 * reset * slow[:, cols] + shift
            decays = jnp.exp(log_decay)
            norm = jnp.sqrt(-jnp.tanh(log_decay) * (decays * decays + 1.0))
            conv = conv.astype(f32)
            dec[:, cols] = decays
            drive[:, cols] = norm * inp * conv
            fac_o[:, cols] = norm * inp
            fac_i[:, cols] = norm * conv * inp * (1.0 - inp)
            fac_r[:, cols] = (-8.0 * slow[:, cols]) * reset * (1.0 - reset)
            grad[:, cols] = inp * conv * decays * decays / norm

    def forward_scan():
        carry = bs_ref[...]
        for i in range(tokens // 8):
            at = slice(8 * i, 8 * i + 8)
            decay = dec[at, :]
            a = decay
            b = drive[at, :]
            for d in (1, 2, 4):
                b = b + a * jnp.where(row >= d, pltpu.roll(b, d, 0), 0.0)
                a = a * jnp.where(row >= d, pltpu.roll(a, d, 0), 1.0)
            state = a * carry + b
            st[at, :] = state
            prev = jnp.where(row >= 1, pltpu.roll(state, 1, 0), carry)
            fac_r[at, :] = fac_r[at, :] * (decay * prev - grad[at, :])
            carry = state[7:8, :]

    def forward_gate():
        for h in range(heads):
            cols = slice(h * head_dim, (h + 1) * head_dim)
            act, slope = gelu_both(gate_ref[:, cols].astype(f32))
            mg[me, :, cols] = (act * st[:, cols]).astype(half)
            act_b[:, cols] = act
            slope_b[:, cols] = st[:, cols] * slope

    def back_products():
        carry_p = jnp.ones((1, total), f32)
        following = jnp.ones((1, total), f32)
        for i in reversed(range(tokens // 8)):
            at = slice(8 * i, 8 * i + 8)
            decay = dec[at, :]
            a = jnp.where(row < 7, pltpu.roll(decay, 7, 0), following)
            following = decay[0:1, :]
            for d, level in ((1, lev0), (2, lev1), (4, lev2)):
                level[at, :] = jnp.where(row < 8 - d, a, 0.0)
                a = a * jnp.where(row < 8 - d, pltpu.roll(a, 8 - d, 0), 1.0)
            drive[at, :] = a
            p = a * carry_p
            prods[at, :] = p
            carry_p = p[0:1, :]

    for copy in loads[4:11]:
        copy.wait()
    forward()
    forward_scan()
    crossed(0)
    relay(0)
    forward_gate()
    back_products()
    for copy in loads[11:]:
        copy.wait()
    grad_chunks = [functools.partial(grads, 0, b) for b in range(parts)]
    steps = [functools.partial(ring, j) for j in range(lines)]
    line_group = per // 2
    for j in range(1, lines):
        arrive(j)
        relay(2 * j - 1)
        if j == max(1, lines - 2):
            steps.pop(0)()
        g = j // line_group
        if j % line_group == 0:
            expert(g - 1)
            if g >= 2:
                join_near(g - 2)
            if g >= 3:
                join_far(g - 3)
        crossed(j)
        relay(2 * j)
        if g > groups // 2 and grad_chunks:
            grad_chunks.pop(0)()
    last = groups - 1
    join_near(last - 1)
    steps.pop(0)()
    relay(n - 1)
    if steps:
        steps.pop(0)()
    expert(last)
    join_far(last - 2)
    join_near(last)
    if steps:
        steps.pop(0)()
    while grad_chunks:
        grad_chunks.pop(0)()
    join_far(last - 1)
    grads(1, 0)
    if steps:
        steps.pop(0)()
    join_far(last)
    for b in range(1, parts):
        grads(1, b)
    lane = lax.broadcasted_iota(jnp.int32, (tokens, 128), 1)
    away = []
    for j in range(top):
        named = upright(info[0, j : j + 1, :]).astype(jnp.int32)
        gap = lax.shift_right_logical(named, 1) - lax.div(me, 2)
        gap = jnp.where(gap < 0, gap + lines, gap)
        away.append(2 * gap + ((named ^ me) & 1))
    member = jnp.zeros((tokens, 128), f32)
    for j in range(top):
        member = jnp.where(away[j] == lane, 1.0, member)
    earlier = lax.broadcasted_iota(jnp.int32, (tokens, tokens), 1) < (
        lax.broadcasted_iota(jnp.int32, (tokens, tokens), 0)
    )
    rank = jnp.dot(
        jnp.where(earlier, 1.0, 0.0).astype(half), member.astype(half), preferred_element_type=f32
    )
    place = lax.broadcasted_iota(jnp.int32, (tokens, n * slots), 1)
    pick_all = jnp.zeros((tokens, n * slots), f32)
    for j in range(top):
        mine = jnp.sum(jnp.where(away[j] == lane, rank, 0.0), axis=1, keepdims=True)
        pick_all = jnp.where(place == away[j] * slots + mine.astype(jnp.int32), 1.0, pick_all)
    pick_all = pick_all.astype(half)
    for k in range(1, n):
        back_copy(k // per, k % per).wait_recv()
    summed = jnp.dot(pick_all, ret[...].reshape(n * slots, width), preferred_element_type=f32)
    dcols[...] = (cot_ref[...].astype(f32) + summed).astype(half)

    some = n // parts
    thin = width // some
    quarter = tokens // parts
    owner_q = lax.div(me, some)

    def blk_copy(i, x):
        peer, part = q * some + i, q ^ x
        at = pl.ds(pl.multiple_of(part * quarter, quarter), quarter)
        return pltpu.make_async_remote_copy(
            src_ref=bsend.at[i, at], dst_ref=got.at[me, at], send_sem=send_sem.at[1],
            recv_sem=blk_sem.at[me], device_id={"sp": peer, "tp": part}, device_id_type=MESH,
        )

    mine_at = pl.ds(pl.multiple_of(q * quarter, quarter), quarter)

    def blk_wait(source):
        spot = got.at[source, mine_at]
        remote(spot, spot, blk_sem.at[source], {"tp": far}).wait_recv()

    def dm_copy(owner, i, other, src):
        return remote(src, dmbuf.at[owner], dm_sem.at[i], {"tp": other})

    start(dm_copy(q, 0, far, dcols))
    start(dm_copy(q, 1, near, dcols))
    for i in range(some):
        bsend[i] = dcols[:, i * thin : (i + 1) * thin]
    for i in range(some):
        for x in range(1, parts):
            start(blk_copy(i, x))

        @pl.when(q * some + i != me)
        def _():
            blk_copy(i, 0).start()

        @pl.when(q * some + i == me)
        def _():
            got[me, mine_at] = bsend[i, mine_at]

    while steps:
        steps.pop(0)()
    dmbuf[q] = dcols[...]

    wo_cols = pl.ds(pl.multiple_of(q * width, width), width)
    grad[...] = against(dcols[...], wo[:, wo_cols])
    dm_copy(far, 0, far, dcols).wait_recv()
    start(dm_copy(far, 2, near, dmbuf.at[far]))
    dm_copy(near, 1, near, dcols).wait_recv()
    dm_copy(near ^ 2, 2, near, dcols).wait_recv()
    for shift_by in (1, 2, 3):
        other = q ^ shift_by
        at = pl.ds(pl.multiple_of(other * width, width), width)
        grad[...] += against(dmbuf[other], wo[:, at])
    carry = jnp.zeros((1, total), f32)
    for i in reversed(range(tokens // 8)):
        at = slice(8 * i, 8 * i + 8)
        b = grad[at, :]
        gate_out_ref[at, :] = (b * slope_b[at, :]).astype(half)
        b = b * act_b[at, :]
        b = b + lev0[at, :] * pltpu.roll(b, 7, 0)
        b = b + lev1[at, :] * pltpu.roll(b, 6, 0)
        b = b + lev2[at, :] * pltpu.roll(b, 4, 0)
        g = drive[at, :] * carry + b
        grad[at, :] = g
        carry = g[0:1, :]
    first = dec[0:1, :]
    mine_pair[0:1, :] = prods[0:1, :] * first
    mine_pair[1:2, :] = carry * first
    mine_pair[2:8, :] = jnp.zeros((6, total), f32)
    pairs[me] = jnp.zeros((8, total), f32)

    def pair_to(peer, source):
        return remote(mine_pair, pairs.at[source], pair_sem.at[source], {"sp": peer})

    for off in range(1, n):
        start(pair_to(lax.rem(me + off, n), me))
    for off in range(1, n):
        blk_wait(lax.rem(me + off, n))

    @pl.when(q != owner_q)
    def _():
        blk_wait(me)

    def got_copy(part, i, other):
        at = pl.ds(pl.multiple_of(part * quarter, quarter), quarter)
        spot = got.at[:, at]
        return remote(spot, spot, got_sem.at[i], {"tp": other})

    start(got_copy(q, 0, far))
    start(got_copy(q, 1, near))

    for off in range(1, n):
        peer = lax.rem(me + off, n)
        pair_to(peer, peer).wait_recv()
    enter = jnp.zeros((1, total), f32)
    for p in reversed(range(n)):
        pair = pairs[p]
        enter = jnp.where(p > me, pair[1:2, :] + pair[0:1, :] * enter, enter)
    for h in range(heads):
        cols = slice(h * head_dim, (h + 1) * head_dim)
        g = grad[:, cols] + prods[:, cols] * enter[:, cols]
        d_r = (g * fac_r[:, cols]).astype(half)
        d_i = (g * fac_i[:, cols]).astype(half)
        out_ref[:, cols] = (
            g * fac_o[:, cols] + against(d_r, wr_ref[h]) + against(d_i, wi_ref[h])
        ).astype(half)
    got_copy(far, 0, far).wait_recv()
    start(got_copy(far, 2, near))
    for j in range(lines):
        spot = mg.at[ring_source(j) ^ 1]
        remote(spot, spot, mx_sem.at[j], {"sp": me ^ 1}).wait_recv()
    got_copy(near, 1, near).wait_recv()
    got_copy(near ^ 2, 2, near).wait_recv()
    go_ref[...] = over(got[...].reshape(n * tokens, thin), mg[...].reshape(n * tokens, width))
    for copy in sent:
        copy.wait_send()
    for i in range(some):

        @pl.when(q * some + i != me)
        def _():
            blk_copy(i, 0).wait_send()


VM = pl.BlockSpec(memory_space=pltpu.VMEM)


def run_whole(
    n, parts, slots, mixed, cot, ids, weights, conv, gate, bs, param, shift, wr, wi, wg, wu, wd, wo
):
    tokens, width = mixed.shape
    full, hidden = wg.shape
    groups = 4
    per = n // groups
    block = per * slots
    some = n // parts
    thin = width // some
    half, f32 = jnp.bfloat16, jnp.float32
    anywhere = pl.BlockSpec(memory_space=pl.ANY)
    dma, vm = pltpu.SemaphoreType.DMA, pltpu.VMEM
    small = (mixed, cot, ids, weights, conv, gate, bs, param, shift, wr, wi)
    return pl.pallas_call(
        functools.partial(whole_kernel, n, groups),
        out_shape=(
            vm((full, hidden), f32), vm((full, hidden), f32), vm((hidden, full), f32),
            vm((thin, width), f32), vm((tokens, width), half), vm((tokens, width), half),
        ),
        in_specs=[anywhere] * 15,
        out_specs=(VM,) * 6,
        scratch_shapes=[vm(a.shape, a.dtype) for a in small] + [
            vm((full, hidden), half), vm((full, hidden), half), vm((hidden, full), half),
            vm((width, full), half),
            vm((n // 2, 8, tokens), f32),
            vm((min(n // 2, 8), 2, tokens, width), half),
            vm((n // 2, 2, slots, width), half),
            vm((parts, n, 2, slots, width), half),
            vm((n * slots, 2 * hidden), half), vm((n * slots, hidden), half),
            vm((groups, parts, block, width), half),
            vm((groups, 2, block, width), half),
            vm((groups, block, width), half),
            vm((groups, block, width), half),
            vm((groups, per, slots, width), half),
            vm((n, slots, width), half),
            vm((tokens, width), half),
            vm((parts, tokens, width), half),
        ] + [vm((tokens, width), f32)] * 13 + [
            vm((n, tokens, width), half),
            vm((n, tokens, thin), half),
            vm((some, tokens, thin), half),
            vm((8, width), f32),
            vm((n, 8, width), f32),
            dma((2,)), dma((n // 2, 2)), pltpu.SemaphoreType.REGULAR, dma((n // 2, 2)), dma((n // 2,)), dma((n // 2,)), dma((n,)), dma((n,)), dma((n,)),
            dma((groups, 2)),
            dma((groups,)), dma((n,)), dma((3,)), dma((15,)),
            dma((n // 2,)), dma((n // 2,)), dma((n,)), dma((3,)), dma((n,)),
        ],
        compiler_params=pltpu.CompilerParams(
            collective_id=0, has_side_effects=True, vmem_limit_bytes=55000 * 1024
        ),
        cost_estimate=pl.CostEstimate(flops=8_000_000_000, bytes_accessed=80_000_000, transcendentals=0),
    )(mixed, cot, ids, weights, conv, gate, bs, param, shift, wr, wi, wg, wu, wd, wo)


def write_kernel(*refs):
    count = len(refs) // 2
    copies = [
        pltpu.make_async_copy(refs[i], refs[count + i], refs[-1].at[i]) for i in range(count)
    ]
    for copy in copies:
        copy.start()
    for copy in copies:
        copy.wait()


def write_out(*arrays):
    held = [pltpu.with_memory_space_constraint(a, pltpu.VMEM) for a in arrays]
    return pl.pallas_call(
        write_kernel,
        out_shape=tuple(jax.ShapeDtypeStruct(a.shape, a.dtype) for a in arrays),
        in_specs=[VM] * len(arrays),
        out_specs=(pl.BlockSpec(memory_space=pl.ANY),) * len(arrays),
        scratch_shapes=[pltpu.SemaphoreType.DMA((len(arrays),))],
        compiler_params=pltpu.CompilerParams(vmem_limit_bytes=1024 * 1024),
    )(*held)


def body(
    conv_out, gate_in, block_states, decay_param, decay_shift, w_reset, w_input, w_out,
    mixed, d_out, expert_ids, route_weights, w_gate, w_up, w_down,
):
    tok_rows, top_k = expert_ids.shape
    experts = lax.axis_size("sp")
    capacity = 2 * tok_rows * top_k // experts
    slots = -(-capacity // 16) * 16
    results = run_whole(
        experts, lax.axis_size("tp"), slots, mixed, d_out, expert_ids.T, route_weights.T,
        conv_out, gate_in, block_states, decay_param[None, :], decay_shift[None, :],
        w_reset, w_input, w_gate[0], w_up[0], w_down[0], w_out,
    )
    grad_gate_e, grad_up_e, grad_down_e, grad_out, grad_in, grad_gate = write_out(*results)
    return (grad_gate_e[None], grad_up_e[None], grad_down_e[None], grad_out, grad_in, grad_gate)


def solution(mesh):
    placed = (
        P("sp", "tp"),
        P("sp", "tp"),
        P("sp", "tp"),
        P("tp"),
        P("sp"),
        P("tp", None, None),
        P("tp", None, None),
        P("tp", None),
        P("sp", "tp"),
        P("sp", "tp"),
        P("sp", None),
        P("sp", None),
        P("sp", None, "tp"),
        P("sp", None, "tp"),
        P("sp", "tp", None),
    )
    return jax.shard_map(
        body,
        mesh=mesh,
        in_specs=placed,
        out_specs=(
            P("sp", None, "tp"),
            P("sp", None, "tp"),
            P("sp", "tp", None),
            P("sp", "tp"),
            P("sp", "tp"),
            P("sp", "tp"),
        ),
        check_vma=False,
    )
```

```python
import functools
import jax
import jax.numpy as jnp
from jax import lax
from jax.experimental import pallas as pl
from jax.experimental.pallas import tpu as pltpu
from jax.sharding import PartitionSpec as P

MESH = pl.DeviceIdType.MESH
GELU_C = 0.7978845608028654
GELU_K = 0.044715


def gelu_both(x):
    inner = jnp.tanh(GELU_C * (x + GELU_K * x * x * x))
    act = 0.5 * x * (1.0 + inner)
    slope = 0.5 * (1.0 + inner) + 0.5 * x * (1.0 - inner * inner) * (
        GELU_C * (1.0 + 3.0 * GELU_K * x * x)
    )
    return act, slope


def softplus_of_negative(x):
    small = jnp.exp(-jnp.abs(x))
    ratio = small / (2.0 + small)
    square = ratio * ratio
    series = jnp.zeros_like(x)
    for odd in range(17, 0, -2):
        series = series * square + 1.0 / odd
    return jnp.maximum(-x, 0.0) + 2.0 * ratio * series


def whole_kernel(
    n, groups,
    mixed_hbm, cot_hbm, ids_hbm, wts_hbm,
    conv_hbm, gate_hbm, bs_hbm, param_hbm, shift_hbm, wr_hbm, wi_hbm,
    wg_hbm, wu_hbm, wd_hbm, wo_hbm,
    acc_g, acc_u, acc_d, go_ref, out_ref, gate_out_ref,
    mixed_ref, cot_ref, ids_ref, wts_ref,
    conv_ref, gate_ref, bs_ref, param_ref, shift_ref, wr_ref, wi_ref,
    wg, wu, wd, wo, info, tok, send, xbuf, dbuf, hbuf, pbuf, nbuf, sbuf, fbuf, rbuf, ret, dcols, dmbuf,
    dec, drive, st, act_b, slope_b, fac_r, fac_i, fac_o, prods, lev0, lev1, lev2, grad,
    mg, got, bsend, bfar, mine_pair, pairs,
    send_sem, tok_send, credit, tok_sem, info_sem, x_sem, y_sem, own_sem, fwd_sem, near_sem, far_sem, ret_sem, dm_sem, w_sem,
    mz_sem, mx_sem, blk_sem, got_sem, pair_sem,
):
    me, q = lax.axis_index("sp"), lax.axis_index("tp")
    near, far = q ^ 1, q ^ 2
    barrier = pltpu.get_barrier_semaphore()
    for off in range(1, n):
        pl.semaphore_signal(
            barrier, inc=1, device_id={"sp": lax.rem(me + off, n)}, device_id_type=MESH
        )
    for other in (near, far):
        pl.semaphore_signal(barrier, inc=1, device_id={"tp": other}, device_id_type=MESH)
    pairs_in = (
        (ids_hbm, ids_ref), (wts_hbm, wts_ref), (mixed_hbm, mixed_ref), (cot_hbm, cot_ref),
        (conv_hbm, conv_ref), (gate_hbm, gate_ref), (bs_hbm, bs_ref), (param_hbm, param_ref),
        (shift_hbm, shift_ref), (wr_hbm, wr_ref), (wi_hbm, wi_ref),
        (wg_hbm, wg), (wu_hbm, wu), (wd_hbm, wd), (wo_hbm, wo),
    )
    loads = [
        pltpu.make_async_copy(src, dst, w_sem.at[i]) for i, (src, dst) in enumerate(pairs_in)
    ]
    for copy in loads:
        copy.start()
    tokens, width = mixed_ref.shape
    top = ids_ref.shape[0]
    slots = send.shape[2]
    hidden = wg.shape[1]
    parts = xbuf.shape[0]
    per = n // groups
    block = per * slots
    heads, head_dim = wr_ref.shape[0], wr_ref.shape[1]
    f32, half = jnp.float32, jnp.bfloat16

    eye = lax.broadcasted_iota(jnp.int32, (tokens, tokens), 0) == (
        lax.broadcasted_iota(jnp.int32, (tokens, tokens), 1)
    )

    def upright(row):
        return jnp.sum(jnp.where(eye, row, jnp.zeros_like(row)), axis=1, keepdims=True)

    for copy in loads[:2]:
        copy.wait()
    for j in range(top):
        info[0, j : j + 1, :] = ids_ref[j : j + 1, :].astype(f32)
        info[0, top + j : top + j + 1, :] = wts_ref[j : j + 1, :]
    info[0, 2 * top :, :] = jnp.zeros((info.shape[1] - 2 * top, tokens), f32)

    def over(left, right):
        return lax.dot_general(left, right, (((0,), (0,)), ((), ())), preferred_element_type=f32)

    def against(left, right):
        return lax.dot_general(left, right, (((1,), (1,)), ((), ())), preferred_element_type=f32)

    sent = []

    def remote(src, dst, recv, where):
        return pltpu.make_async_remote_copy(
            src_ref=src, dst_ref=dst, send_sem=send_sem.at[0], recv_sem=recv,
            device_id=where, device_id_type=MESH,
        )

    def start(copy):
        copy.start()
        sent.append(copy)

    lines, held = n // 2, tok.shape[0]
    following_line = lax.rem(me + 2, n)

    def ring_copy(j, i):
        source = (mixed_hbm, cot_hbm)[i] if j == 0 else tok.at[j % held, i]
        return pltpu.make_async_remote_copy(
            src_ref=source, dst_ref=tok.at[(j + 1) % held, i], send_sem=tok_send.at[j, i],
            recv_sem=tok_sem.at[j + 1, i], device_id={"sp": following_line}, device_id_type=MESH,
        )

    def ring_start(j):
        if j + 1 > held:
            pl.semaphore_wait(credit, 1)
        for i in range(2):
            ring_copy(j, i).start()

    def ring_free(j):
        for i in range(2):
            ring_copy(j, i).wait_send()
        if 1 <= j and j + held < lines:
            pl.semaphore_signal(
                credit, inc=1, device_id={"sp": lax.rem(me + n - 2, n)}, device_id_type=MESH
            )

    def info_copy(j):
        return remote(info.at[0], info.at[j], info_sem.at[j], {"sp": lax.rem(me + 2 * j, n)})

    def cross_copy(j):
        return remote(send.at[j], xbuf.at[q, 2 * j + 1], x_sem.at[j], {"sp": me ^ 1})

    slot = lax.broadcasted_iota(jnp.int32, (slots, tokens), 0)
    before = lax.broadcasted_iota(jnp.int32, (tokens, tokens), 0) < (
        lax.broadcasted_iota(jnp.int32, (tokens, tokens), 1)
    )

    def arrive(j):
        if j > 0:
            for i in range(2):
                ring_copy(j - 1, i).wait_recv()
            if j < lines - 1:
                ring_start(j)
            info_copy(j).wait_recv()
        rows = mixed_ref[...] if j == 0 else tok[j % held, 0]
        cots = cot_ref[...] if j == 0 else tok[j % held, 1]
        ids = [info[j, i : i + 1, :].astype(jnp.int32) for i in range(top)]
        which = lax.broadcasted_iota(jnp.int32, (8, tokens), 0)
        wanted = jnp.where(which == 0, me, me ^ 1)
        hit = jnp.zeros((8, tokens), f32)
        weight = jnp.zeros((8, tokens), f32)
        for i in range(top):
            same = ids[i] == wanted
            hit = jnp.where(same, 1.0, hit)
            weight = jnp.where(same, info[j, top + i : top + i + 1, :], weight)
        order = jnp.dot(
            hit.astype(half), jnp.where(before, 1.0, 0.0).astype(half), preferred_element_type=f32
        )
        order = jnp.where(hit > 0.5, order, -1.0).astype(jnp.int32)
        for side in (1, 0):
            chosen = slot == order[side : side + 1, :]
            pick = jnp.where(chosen, 1.0, 0.0).astype(half)
            scale = jnp.sum(
                jnp.where(chosen, weight[side : side + 1, :], 0.0), axis=1, keepdims=True
            )
            x = jnp.dot(pick, rows, preferred_element_type=f32).astype(half)
            c = (scale * jnp.dot(pick, cots, preferred_element_type=f32)).astype(half)
            if side == 1:
                send[j, 0] = x
                send[j, 1] = c
                start(cross_copy(j))
            else:
                xbuf[q, 2 * j, 0] = x
                xbuf[q, 2 * j, 1] = c
                spread(2 * j)
        if j > 0:
            ring_free(j - 1)

    def crossed(j):
        cross_copy(j).wait_recv()
        spread(2 * j + 1)

    def over_tp(owner, k, other, sems):
        spot = xbuf.at[owner, k]
        return remote(spot, spot, sems.at[k], {"tp": other})

    def spread(k):
        start(over_tp(q, k, far, y_sem))
        start(over_tp(q, k, near, own_sem))

    def relay(k):
        over_tp(far, k, far, y_sem).wait_recv()
        start(over_tp(far, k, near, fwd_sem))

    def near_copy(g, i):
        return remote(
            pbuf.at[g, near if i == 0 else far ^ 1], nbuf.at[g, i], near_sem.at[g, i], {"tp": near}
        )

    def expert(g):
        for k in range(g * per, (g + 1) * per):
            over_tp(near, k, near, own_sem).wait_recv()
            over_tp(near ^ 2, k, near, fwd_sem).wait_recv()
        here = slice(g * per, (g + 1) * per)
        up_pre = jnp.zeros((block, hidden), f32)
        linear = jnp.zeros((block, hidden), f32)
        d_hidden = jnp.zeros((block, hidden), f32)
        for b in range(parts):
            cols = slice(b * width, (b + 1) * width)
            x = xbuf[b, here, 0].reshape(block, width)
            c = xbuf[b, here, 1].reshape(block, width)
            up_pre += jnp.dot(x, wg[cols, :], preferred_element_type=f32)
            linear += jnp.dot(x, wu[cols, :], preferred_element_type=f32)
            d_hidden += against(c, wd[:, cols])
        sig = jax.nn.sigmoid(up_pre)
        silu = up_pre * sig
        rows = slice(g * block, (g + 1) * block)
        hbuf[rows, :] = (silu * linear).astype(half)
        d_linear = (d_hidden * silu).astype(half)
        d_up = (d_hidden * linear * sig * (1.0 + up_pre * (1.0 - sig))).astype(half)
        dbuf[rows, :hidden] = d_up
        dbuf[rows, hidden:] = d_linear
        for b in range(parts):
            cols = slice(b * width, (b + 1) * width)
            pbuf[g, b] = (against(d_up, wg[cols, :]) + against(d_linear, wu[cols, :])).astype(half)
        for i in range(2):
            start(near_copy(g, 1 - i))

    def far_copy(g):
        return remote(sbuf.at[g], fbuf.at[g], far_sem.at[g], {"tp": far})

    def join_near(g):
        near_copy(g, 1).wait_recv()
        sbuf[g] = (pbuf[g, far].astype(f32) + nbuf[g, 1].astype(f32)).astype(half)
        start(far_copy(g))

    def back_copy(g, i):
        k = g * per + i
        return remote(
            rbuf.at[g, i], ret.at[k], ret_sem.at[k],
            {"sp": lax.rem(me + n - 2 * (k // 2), n) ^ (k % 2)},
        )

    def join_far(g):
        near_copy(g, 0).wait_recv()
        far_copy(g).wait_recv()
        whole = pbuf[g, q].astype(f32) + nbuf[g, 0].astype(f32) + fbuf[g].astype(f32)
        rbuf[g] = whole.astype(half).reshape(per, slots, width)
        for i in range(per):
            if g * per + i > 0:
                start(back_copy(g, i))
        if g == 0:
            ret[0] = whole[:slots].astype(half)

    def grads(h, b):
        some = n // 2
        here = slice(h * some, (h + 1) * some)
        rows = slice(h * some * slots, (h + 1) * some * slots)
        cols = slice(b * width, (b + 1) * width)
        both = over(xbuf[b, here, 0].reshape(some * slots, width), dbuf[rows, :])
        down = over(hbuf[rows, :], xbuf[b, here, 1].reshape(some * slots, width))
        if h == 0:
            acc_g[cols, :] = both[:, :hidden]
            acc_u[cols, :] = both[:, hidden:]
            acc_d[:, cols] = down
        else:
            acc_g[cols, :] += both[:, :hidden]
            acc_u[cols, :] += both[:, hidden:]
            acc_d[:, cols] += down

    def ring_source(j):
        return lax.rem(me + n - 2 * j, n)

    def ring_send(j, source):
        start(remote(mg.at[source], mg.at[source], mx_sem.at[j], {"sp": me ^ 1}))
        if j < lines - 1:
            start(remote(mg.at[source], mg.at[source], mz_sem.at[j + 1], {"sp": lax.rem(me + 2, n)}))

    def ring(j):
        source = ring_source(j)
        spot = mg.at[source]
        if j > 0:
            remote(spot, spot, mz_sem.at[j], {"sp": me ^ 1}).wait_recv()
        ring_send(j, source)

    pl.semaphore_wait(barrier, n + 1)
    ring_start(0)
    for j in range(1, lines):
        start(info_copy(j))
    for copy in loads[2:4]:
        copy.wait()
    arrive(0)

    total = width
    row = lax.broadcasted_iota(jnp.int32, (8, total), 0)

    def forward():
        slow = softplus_of_negative(param_ref[...])
        shift = upright(shift_ref[...])
        for h in range(heads):
            cols = slice(h * head_dim, (h + 1) * head_dim)
            conv = conv_ref[:, cols]
            reset = jax.nn.sigmoid(jnp.dot(conv, wr_ref[h], preferred_element_type=f32))
            inp = jax.nn.sigmoid(jnp.dot(conv, wi_ref[h], preferred_element_type=f32))
            log_decay = -8.0 * reset * slow[:, cols] + shift
            decays = jnp.exp(log_decay)
            norm = jnp.sqrt(-jnp.tanh(log_decay) * (decays * decays + 1.0))
            conv = conv.astype(f32)
            dec[:, cols] = decays
            drive[:, cols] = norm * inp * conv
            fac_o[:, cols] = norm * inp
            fac_i[:, cols] = norm * conv * inp * (1.0 - inp)
            fac_r[:, cols] = (-8.0 * slow[:, cols]) * reset * (1.0 - reset)
            grad[:, cols] = inp * conv * decays * decays / norm

    def forward_scan():
        carry = bs_ref[...]
        for i in range(tokens // 8):
            at = slice(8 * i, 8 * i + 8)
            decay = dec[at, :]
            a = decay
            b = drive[at, :]
            for d in (1, 2, 4):
                b = b + a * jnp.where(row >= d, pltpu.roll(b, d, 0), 0.0)
                a = a * jnp.where(row >= d, pltpu.roll(a, d, 0), 1.0)
            state = a * carry + b
            st[at, :] = state
            prev = jnp.where(row >= 1, pltpu.roll(state, 1, 0), carry)
            fac_r[at, :] = fac_r[at, :] * (decay * prev - grad[at, :])
            carry = state[7:8, :]

    def forward_gate():
        for h in range(heads):
            cols = slice(h * head_dim, (h + 1) * head_dim)
            act, slope = gelu_both(gate_ref[:, cols].astype(f32))
            mg[me, :, cols] = (act * st[:, cols]).astype(half)
            act_b[:, cols] = act
            slope_b[:, cols] = st[:, cols] * slope

    def back_products():
        carry_p = jnp.ones((1, total), f32)
        following = jnp.ones((1, total), f32)
        for i in reversed(range(tokens // 8)):
            at = slice(8 * i, 8 * i + 8)
            decay = dec[at, :]
            a = jnp.where(row < 7, pltpu.roll(decay, 7, 0), following)
            following = decay[0:1, :]
            for d, level in ((1, lev0), (2, lev1), (4, lev2)):
                level[at, :] = jnp.where(row < 8 - d, a, 0.0)
                a = a * jnp.where(row < 8 - d, pltpu.roll(a, 8 - d, 0), 1.0)
            drive[at, :] = a
            p = a * carry_p
            prods[at, :] = p
            carry_p = p[0:1, :]

    for copy in loads[4:11]:
        copy.wait()
    forward()
    forward_scan()
    crossed(0)
    relay(0)
    forward_gate()
    back_products()
    for copy in loads[11:]:
        copy.wait()
    grad_chunks = [functools.partial(grads, h, b) for h in range(2) for b in range(parts)]
    steps = [functools.partial(ring, j) for j in range(lines)]

    def some_of(work, count):
        for _ in range(min(count, len(work))):
            work.pop(0)()

    line_group = per // 2
    for j in range(1, lines):
        g = j // line_group if j % line_group == 0 else 0
        arrive(j)
        if g == 3:
            join_far(1)
        relay(2 * j - 1)
        if j == max(1, lines - 2) or g == 3:
            some_of(steps, 1)
        if g:
            expert(g - 1)
        if g == 2:
            join_near(1)
        crossed(j)
        relay(2 * j)
    join_near(2)
    relay(n - 1)
    some_of(steps, 1)
    expert(3)
    join_near(3)
    join_near(0)
    join_far(2)
    some_of(grad_chunks, 4)
    some_of(steps, 1)
    join_far(3)
    some_of(grad_chunks, 4)
    join_far(0)
    lane = lax.broadcasted_iota(jnp.int32, (tokens, 128), 1)
    away = []
    for j in range(top):
        named = upright(info[0, j : j + 1, :]).astype(jnp.int32)
        gap = lax.shift_right_logical(named, 1) - lax.div(me, 2)
        gap = jnp.where(gap < 0, gap + lines, gap)
        away.append(2 * gap + ((named ^ me) & 1))
    member = jnp.zeros((tokens, 128), f32)
    for j in range(top):
        member = jnp.where(away[j] == lane, 1.0, member)
    earlier = lax.broadcasted_iota(jnp.int32, (tokens, tokens), 1) < (
        lax.broadcasted_iota(jnp.int32, (tokens, tokens), 0)
    )
    rank = jnp.dot(
        jnp.where(earlier, 1.0, 0.0).astype(half), member.astype(half), preferred_element_type=f32
    )
    place = lax.broadcasted_iota(jnp.int32, (tokens, n * slots), 1)
    pick_all = jnp.zeros((tokens, n * slots), f32)
    for j in range(top):
        mine = jnp.sum(jnp.where(away[j] == lane, rank, 0.0), axis=1, keepdims=True)
        pick_all = jnp.where(place == away[j] * slots + mine.astype(jnp.int32), 1.0, pick_all)
    pick_all = pick_all.astype(half)
    for k in range(1, n):
        back_copy(k // per, k % per).wait_recv()
    summed = jnp.dot(pick_all, ret[...].reshape(n * slots, width), preferred_element_type=f32)
    dcols[...] = (cot_ref[...].astype(f32) + summed).astype(half)

    some = n // parts
    thin = width // some
    big, little = tokens // 3, tokens // 6
    owner = lax.div(me, some)
    apart = q ^ owner
    place_in = apart & 1

    def blk_copy(source, i, peer, other, first, size):
        return pltpu.make_async_remote_copy(
            src_ref=source.at[i, first : first + size],
            dst_ref=got.at[me, pl.ds(first, size)],
            send_sem=send_sem.at[1], recv_sem=blk_sem.at[me],
            device_id={"sp": peer, "tp": other}, device_id_type=MESH,
        )

    blocks_sent = []

    def blk_send(source, held, first, size):
        for i in range(some):
            peer = held * some + i
            start(blk_copy(source, i, peer, near, first + size, size))
            mine = blk_copy(source, i, peer, q, first, size)
            blocks_sent.append((peer, mine))

            @pl.when(peer != me)
            def _():
                mine.start()

            @pl.when(peer == me)
            def _():
                got[me, first : first + size] = source[i, first : first + size]

    def rows_big(part):
        return pl.ds(pl.multiple_of(part * big, big), big)

    def rows_little(part):
        return pl.ds(pl.multiple_of(2 * big + part * little, little), little)

    def rows_of(mine, part, inside):
        return rows_big(part) if mine == inside else rows_little(part)

    def got_copy(inside, mine, part, i, other):
        spot = got.at[:, rows_of(mine, part, inside)]
        return pltpu.make_async_remote_copy(
            src_ref=spot, dst_ref=spot, send_sem=send_sem.at[1], recv_sem=got_sem.at[i],
            device_id={"tp": other}, device_id_type=MESH,
        )

    def share(inside):
        spot_rows = rows_of(True, place_in, inside)
        for off in range(1, n):
            source = lax.rem(me + off, n)
            spot = got.at[source, spot_rows]
            remote(spot, spot, blk_sem.at[source], {"tp": far}).wait_recv()

        @pl.when(place_in == 1)
        def _():
            spot = got.at[me, spot_rows]
            remote(spot, spot, blk_sem.at[me], {"tp": far}).wait_recv()

        got_copy(inside, True, place_in, 0, far).start()
        got_copy(inside, True, place_in, 1, near).start()

    def share_on(inside):
        got_copy(inside, False, place_in, 0, far).wait_recv()
        got_copy(inside, False, place_in, 2, near).start()

    def project(inside, mine, part):
        at = rows_of(mine, part, inside)
        count = n * (big if mine == inside else little)
        return over(got[:, at, :].reshape(count, thin), mg[:, at, :].reshape(count, width))

    def project_own(inside):
        go_ref[...] = project(inside, True, place_in)

    def project_rest(inside):
        go_ref[...] += project(inside, False, place_in)
        got_copy(inside, True, place_in ^ 1, 1, near).wait_recv()
        go_ref[...] += project(inside, True, place_in ^ 1)
        got_copy(inside, False, place_in ^ 1, 2, near).wait_recv()
        go_ref[...] += project(inside, False, place_in ^ 1)
        for i, other in ((0, far), (1, near)):
            got_copy(inside, True, place_in, i, other).wait_send()
        got_copy(inside, False, place_in, 2, near).wait_send()

    def each(work, *sides):
        for inside in sides:
            pl.when((apart < 2) == inside)(functools.partial(work, inside))

    def dm_copy(owner, i, other, src):
        return remote(src, dmbuf.at[owner], dm_sem.at[i], {"tp": other})

    start(dm_copy(q, 0, far, dcols))
    start(dm_copy(q, 1, near, dcols))
    for i in range(some):
        bsend[i] = dcols[:, i * thin : (i + 1) * thin]
    blk_send(bsend, q, 0, big)
    while steps:
        steps.pop(0)()
    dmbuf[q] = dcols[...]

    wo_cols = pl.ds(pl.multiple_of(q * width, width), width)
    grad[...] = against(dcols[...], wo[:, wo_cols])
    dm_copy(far, 0, far, dcols).wait_recv()
    start(dm_copy(far, 2, near, dmbuf.at[far]))
    for i in range(some):
        bfar[i, 2 * big :, :] = dmbuf[far, 2 * big :, i * thin : (i + 1) * thin]
    blk_send(bfar, far, 2 * big, little)
    dm_copy(near, 1, near, dcols).wait_recv()
    dm_copy(near ^ 2, 2, near, dcols).wait_recv()
    for shift_by in (1, 2, 3):
        other = q ^ shift_by
        at = pl.ds(pl.multiple_of(other * width, width), width)
        grad[...] += against(dmbuf[other], wo[:, at])
    each(share, True)
    carry = jnp.zeros((1, total), f32)
    for i in reversed(range(tokens // 8)):
        at = slice(8 * i, 8 * i + 8)
        b = grad[at, :]
        gate_out_ref[at, :] = (b * slope_b[at, :]).astype(half)
        b = b * act_b[at, :]
        b = b + lev0[at, :] * pltpu.roll(b, 7, 0)
        b = b + lev1[at, :] * pltpu.roll(b, 6, 0)
        b = b + lev2[at, :] * pltpu.roll(b, 4, 0)
        g = drive[at, :] * carry + b
        grad[at, :] = g
        carry = g[0:1, :]
    first = dec[0:1, :]
    mine_pair[0:1, :] = prods[0:1, :] * first
    mine_pair[1:2, :] = carry * first
    mine_pair[2:8, :] = jnp.zeros((6, total), f32)
    pairs[me] = jnp.zeros((8, total), f32)

    def pair_to(peer, source):
        return remote(mine_pair, pairs.at[source], pair_sem.at[source], {"sp": peer})

    for off in range(1, n):
        start(pair_to(lax.rem(me + off, n), me))
    each(share, False)
    for j in range(lines):
        spot = mg.at[ring_source(j) ^ 1]
        remote(spot, spot, mx_sem.at[j], {"sp": me ^ 1}).wait_recv()
    each(project_own, True, False)
    for off in range(1, n):
        peer = lax.rem(me + off, n)
        pair_to(peer, peer).wait_recv()
    enter = jnp.zeros((1, total), f32)
    each(share_on, True, False)
    for p in reversed(range(n)):
        pair = pairs[p]
        enter = jnp.where(p > me, pair[1:2, :] + pair[0:1, :] * enter, enter)
    for h in range(heads):
        cols = slice(h * head_dim, (h + 1) * head_dim)
        g = grad[:, cols] + prods[:, cols] * enter[:, cols]
        d_r = (g * fac_r[:, cols]).astype(half)
        d_i = (g * fac_i[:, cols]).astype(half)
        out_ref[:, cols] = (
            g * fac_o[:, cols] + against(d_r, wr_ref[h]) + against(d_i, wi_ref[h])
        ).astype(half)
    each(project_rest, True, False)
    for copy in sent:
        copy.wait_send()
    for peer, copy in blocks_sent:

        @pl.when(peer != me)
        def _():
            copy.wait_send()


VM = pl.BlockSpec(memory_space=pltpu.VMEM)


def run_whole(
    n, parts, slots, mixed, cot, ids, weights, conv, gate, bs, param, shift, wr, wi, wg, wu, wd, wo
):
    tokens, width = mixed.shape
    full, hidden = wg.shape
    groups = 4
    per = n // groups
    block = per * slots
    some = n // parts
    thin = width // some
    half, f32 = jnp.bfloat16, jnp.float32
    anywhere = pl.BlockSpec(memory_space=pl.ANY)
    dma, vm = pltpu.SemaphoreType.DMA, pltpu.VMEM
    small = (mixed, cot, ids, weights, conv, gate, bs, param, shift, wr, wi)
    return pl.pallas_call(
        functools.partial(whole_kernel, n, groups),
        out_shape=(
            vm((full, hidden), f32), vm((full, hidden), f32), vm((hidden, full), f32),
            vm((thin, width), f32), vm((tokens, width), half), vm((tokens, width), half),
        ),
        in_specs=[anywhere] * 15,
        out_specs=(VM,) * 6,
        scratch_shapes=[vm(a.shape, a.dtype) for a in small] + [
            vm((full, hidden), half), vm((full, hidden), half), vm((hidden, full), half),
            vm((width, full), half),
            vm((n // 2, 8, tokens), f32),
            vm((min(n // 2, 8), 2, tokens, width), half),
            vm((n // 2, 2, slots, width), half),
            vm((parts, n, 2, slots, width), half),
            vm((n * slots, 2 * hidden), half), vm((n * slots, hidden), half),
            vm((groups, parts, block, width), half),
            vm((groups, 2, block, width), half),
            vm((groups, block, width), half),
            vm((groups, block, width), half),
            vm((groups, per, slots, width), half),
            vm((n, slots, width), half),
            vm((tokens, width), half),
            vm((parts, tokens, width), half),
        ] + [vm((tokens, width), f32)] * 13 + [
            vm((n, tokens, width), half),
            vm((n, tokens, thin), half),
            vm((some, tokens, thin), half),
            vm((some, tokens, thin), half),
            vm((8, width), f32),
            vm((n, 8, width), f32),
            dma((2,)), dma((n // 2, 2)), pltpu.SemaphoreType.REGULAR, dma((n // 2, 2)), dma((n // 2,)), dma((n // 2,)), dma((n,)), dma((n,)), dma((n,)),
            dma((groups, 2)),
            dma((groups,)), dma((n,)), dma((3,)), dma((15,)),
            dma((n // 2,)), dma((n // 2,)), dma((n,)), dma((3,)), dma((n,)),
        ],
        compiler_params=pltpu.CompilerParams(
            collective_id=0, has_side_effects=True, vmem_limit_bytes=57000 * 1024
        ),
        cost_estimate=pl.CostEstimate(flops=8_000_000_000, bytes_accessed=80_000_000, transcendentals=0),
    )(mixed, cot, ids, weights, conv, gate, bs, param, shift, wr, wi, wg, wu, wd, wo)


def write_kernel(*refs):
    count = len(refs) // 2
    copies = [
        pltpu.make_async_copy(refs[i], refs[count + i], refs[-1].at[i]) for i in range(count)
    ]
    for copy in copies:
        copy.start()
    for copy in copies:
        copy.wait()


def write_out(*arrays):
    held = [pltpu.with_memory_space_constraint(a, pltpu.VMEM) for a in arrays]
    return pl.pallas_call(
        write_kernel,
        out_shape=tuple(jax.ShapeDtypeStruct(a.shape, a.dtype) for a in arrays),
        in_specs=[VM] * len(arrays),
        out_specs=(pl.BlockSpec(memory_space=pl.ANY),) * len(arrays),
        scratch_shapes=[pltpu.SemaphoreType.DMA((len(arrays),))],
        compiler_params=pltpu.CompilerParams(vmem_limit_bytes=1024 * 1024),
    )(*held)


def body(
    conv_out, gate_in, block_states, decay_param, decay_shift, w_reset, w_input, w_out,
    mixed, d_out, expert_ids, route_weights, w_gate, w_up, w_down,
):
    tok_rows, top_k = expert_ids.shape
    experts = lax.axis_size("sp")
    capacity = 2 * tok_rows * top_k // experts
    slots = -(-capacity // 16) * 16
    results = run_whole(
        experts, lax.axis_size("tp"), slots, mixed, d_out, expert_ids.T, route_weights.T,
        conv_out, gate_in, block_states, decay_param[None, :], decay_shift[None, :],
        w_reset, w_input, w_gate[0], w_up[0], w_down[0], w_out,
    )
    grad_gate_e, grad_up_e, grad_down_e, grad_out, grad_in, grad_gate = write_out(*results)
    return (grad_gate_e[None], grad_up_e[None], grad_down_e[None], grad_out, grad_in, grad_gate)


def solution(mesh):
    placed = (
        P("sp", "tp"),
        P("sp", "tp"),
        P("sp", "tp"),
        P("tp"),
        P("sp"),
        P("tp", None, None),
        P("tp", None, None),
        P("tp", None),
        P("sp", "tp"),
        P("sp", "tp"),
        P("sp", None),
        P("sp", None),
        P("sp", None, "tp"),
        P("sp", None, "tp"),
        P("sp", "tp", None),
    )
    return jax.shard_map(
        body,
        mesh=mesh,
        in_specs=placed,
        out_specs=(
            P("sp", None, "tp"),
            P("sp", None, "tp"),
            P("sp", "tp", None),
            P("sp", "tp"),
            P("sp", "tp"),
            P("sp", "tp"),
        ),
        check_vma=False,
    )
```

```python
import functools
import jax
import jax.numpy as jnp
from jax import lax
from jax.experimental import pallas as pl
from jax.experimental.pallas import tpu as pltpu
from jax.sharding import PartitionSpec as P

MESH = pl.DeviceIdType.MESH
GELU_C = 0.7978845608028654
GELU_K = 0.044715


def gelu_both(x):
    inner = jnp.tanh(GELU_C * (x + GELU_K * x * x * x))
    act = 0.5 * x * (1.0 + inner)
    slope = 0.5 * (1.0 + inner) + 0.5 * x * (1.0 - inner * inner) * (
        GELU_C * (1.0 + 3.0 * GELU_K * x * x)
    )
    return act, slope


def softplus_of_negative(x):
    small = jnp.exp(-jnp.abs(x))
    ratio = small / (2.0 + small)
    square = ratio * ratio
    series = jnp.zeros_like(x)
    for odd in range(17, 0, -2):
        series = series * square + 1.0 / odd
    return jnp.maximum(-x, 0.0) + 2.0 * ratio * series


def whole_kernel(
    n, groups,
    mixed_hbm, cot_hbm, ids_hbm, wts_hbm,
    conv_hbm, gate_hbm, bs_hbm, param_hbm, shift_hbm, wr_hbm, wi_hbm,
    wg_hbm, wu_hbm, wd_hbm, wo_hbm,
    acc_g, acc_u, acc_d, go_ref, out_ref, gate_out_ref,
    mixed_ref, cot_ref, ids_ref, wts_ref,
    conv_ref, gate_ref, bs_ref, param_ref, shift_ref, wr_ref, wi_ref,
    wg, wu, wd, wo, info, tok, send, xbuf, dbuf, hbuf, pbuf, nbuf, sbuf, fbuf, rbuf, ret, dcols, dmbuf,
    dec, drive, st, act_b, slope_b, fac_r, fac_i, fac_o, prods, lev0, lev1, lev2, grad,
    mg, got, bsend, bfar, mine_pair, pairs,
    send_sem, tok_send, credit, tok_sem, info_sem, x_sem, y_sem, own_sem, fwd_sem, near_sem, far_sem, ret_sem, dm_sem, w_sem,
    mz_sem, mx_sem, blk_sem, got_sem, pair_sem,
):
    me, q = lax.axis_index("sp"), lax.axis_index("tp")
    near, far = q ^ 1, q ^ 2
    barrier = pltpu.get_barrier_semaphore()
    for off in range(1, n):
        pl.semaphore_signal(
            barrier, inc=1, device_id={"sp": lax.rem(me + off, n)}, device_id_type=MESH
        )
    for other in (near, far):
        pl.semaphore_signal(barrier, inc=1, device_id={"tp": other}, device_id_type=MESH)
    pairs_in = (
        (ids_hbm, ids_ref), (wts_hbm, wts_ref), (mixed_hbm, mixed_ref), (cot_hbm, cot_ref),
        (conv_hbm, conv_ref), (gate_hbm, gate_ref), (bs_hbm, bs_ref), (param_hbm, param_ref),
        (shift_hbm, shift_ref), (wr_hbm, wr_ref), (wi_hbm, wi_ref),
        (wg_hbm, wg), (wu_hbm, wu), (wd_hbm, wd), (wo_hbm, wo),
    )
    loads = [
        pltpu.make_async_copy(src, dst, w_sem.at[i]) for i, (src, dst) in enumerate(pairs_in)
    ]
    for copy in loads:
        copy.start()
    tokens, width = mixed_ref.shape
    top = ids_ref.shape[0]
    slots = send.shape[2]
    hidden = wg.shape[1]
    parts = xbuf.shape[0]
    per = n // groups
    block = per * slots
    heads, head_dim = wr_ref.shape[0], wr_ref.shape[1]
    f32, half = jnp.float32, jnp.bfloat16

    eye = lax.broadcasted_iota(jnp.int32, (tokens, tokens), 0) == (
        lax.broadcasted_iota(jnp.int32, (tokens, tokens), 1)
    )

    def upright(row):
        return jnp.sum(jnp.where(eye, row, jnp.zeros_like(row)), axis=1, keepdims=True)

    for copy in loads[:2]:
        copy.wait()
    for j in range(top):
        info[0, j : j + 1, :] = ids_ref[j : j + 1, :].astype(f32)
        info[0, top + j : top + j + 1, :] = wts_ref[j : j + 1, :]
    info[0, 2 * top :, :] = jnp.zeros((info.shape[1] - 2 * top, tokens), f32)

    def over(left, right):
        return lax.dot_general(left, right, (((0,), (0,)), ((), ())), preferred_element_type=f32)

    def against(left, right):
        return lax.dot_general(left, right, (((1,), (1,)), ((), ())), preferred_element_type=f32)

    sent = []

    def remote(src, dst, recv, where):
        return pltpu.make_async_remote_copy(
            src_ref=src, dst_ref=dst, send_sem=send_sem.at[0], recv_sem=recv,
            device_id=where, device_id_type=MESH,
        )

    def start(copy):
        copy.start()
        sent.append(copy)

    lines, held = n // 2, tok.shape[0]
    following_line = lax.rem(me + 2, n)

    def ring_copy(j, i):
        source = (mixed_hbm, cot_hbm)[i] if j == 0 else tok.at[j % held, i]
        return pltpu.make_async_remote_copy(
            src_ref=source, dst_ref=tok.at[(j + 1) % held, i], send_sem=tok_send.at[j, i],
            recv_sem=tok_sem.at[j + 1, i], device_id={"sp": following_line}, device_id_type=MESH,
        )

    def ring_start(j):
        if j + 1 > held:
            pl.semaphore_wait(credit, 1)
        for i in range(2):
            ring_copy(j, i).start()

    def ring_free(j):
        for i in range(2):
            ring_copy(j, i).wait_send()
        if 1 <= j and j + held < lines:
            pl.semaphore_signal(
                credit, inc=1, device_id={"sp": lax.rem(me + n - 2, n)}, device_id_type=MESH
            )

    def info_copy(j):
        return remote(info.at[0], info.at[j], info_sem.at[j], {"sp": lax.rem(me + 2 * j, n)})

    def cross_copy(j):
        return remote(send.at[j], xbuf.at[q, 2 * j + 1], x_sem.at[j], {"sp": me ^ 1})

    slot = lax.broadcasted_iota(jnp.int32, (slots, tokens), 0)
    before = lax.broadcasted_iota(jnp.int32, (tokens, tokens), 0) < (
        lax.broadcasted_iota(jnp.int32, (tokens, tokens), 1)
    )

    def arrive(j):
        if j > 0:
            for i in range(2):
                ring_copy(j - 1, i).wait_recv()
            if j < lines - 1:
                ring_start(j)
            info_copy(j).wait_recv()
        rows = mixed_ref[...] if j == 0 else tok[j % held, 0]
        cots = cot_ref[...] if j == 0 else tok[j % held, 1]
        ids = [info[j, i : i + 1, :].astype(jnp.int32) for i in range(top)]
        which = lax.broadcasted_iota(jnp.int32, (8, tokens), 0)
        wanted = jnp.where(which == 0, me, me ^ 1)
        hit = jnp.zeros((8, tokens), f32)
        weight = jnp.zeros((8, tokens), f32)
        for i in range(top):
            same = ids[i] == wanted
            hit = jnp.where(same, 1.0, hit)
            weight = jnp.where(same, info[j, top + i : top + i + 1, :], weight)
        order = jnp.dot(
            hit.astype(half), jnp.where(before, 1.0, 0.0).astype(half), preferred_element_type=f32
        )
        order = jnp.where(hit > 0.5, order, -1.0).astype(jnp.int32)
        for side in (1, 0):
            chosen = slot == order[side : side + 1, :]
            pick = jnp.where(chosen, 1.0, 0.0).astype(half)
            scale = jnp.sum(
                jnp.where(chosen, weight[side : side + 1, :], 0.0), axis=1, keepdims=True
            )
            x = jnp.dot(pick, rows, preferred_element_type=f32).astype(half)
            c = (scale * jnp.dot(pick, cots, preferred_element_type=f32)).astype(half)
            if side == 1:
                send[j, 0] = x
                send[j, 1] = c
                start(cross_copy(j))
            else:
                xbuf[q, 2 * j, 0] = x
                xbuf[q, 2 * j, 1] = c
                spread(2 * j)
        if j > 0:
            ring_free(j - 1)

    def crossed(j):
        cross_copy(j).wait_recv()
        spread(2 * j + 1)

    def over_tp(owner, k, other, sems):
        spot = xbuf.at[owner, k]
        return remote(spot, spot, sems.at[k], {"tp": other})

    def spread(k):
        start(over_tp(q, k, far, y_sem))
        start(over_tp(q, k, near, own_sem))

    def relay(k):
        over_tp(far, k, far, y_sem).wait_recv()
        start(over_tp(far, k, near, fwd_sem))

    def near_copy(g, i):
        return remote(
            pbuf.at[g, near if i == 0 else far ^ 1], nbuf.at[g, i], near_sem.at[g, i], {"tp": near}
        )

    def expert(g):
        for k in range(g * per, (g + 1) * per):
            over_tp(near, k, near, own_sem).wait_recv()
            over_tp(near ^ 2, k, near, fwd_sem).wait_recv()
        here = slice(g * per, (g + 1) * per)
        up_pre = jnp.zeros((block, hidden), f32)
        linear = jnp.zeros((block, hidden), f32)
        d_hidden = jnp.zeros((block, hidden), f32)
        for b in range(parts):
            cols = slice(b * width, (b + 1) * width)
            x = xbuf[b, here, 0].reshape(block, width)
            c = xbuf[b, here, 1].reshape(block, width)
            up_pre += jnp.dot(x, wg[cols, :], preferred_element_type=f32)
            linear += jnp.dot(x, wu[cols, :], preferred_element_type=f32)
            d_hidden += against(c, wd[:, cols])
        sig = jax.nn.sigmoid(up_pre)
        silu = up_pre * sig
        rows = slice(g * block, (g + 1) * block)
        hbuf[rows, :] = (silu * linear).astype(half)
        d_linear = (d_hidden * silu).astype(half)
        d_up = (d_hidden * linear * sig * (1.0 + up_pre * (1.0 - sig))).astype(half)
        dbuf[rows, :hidden] = d_up
        dbuf[rows, hidden:] = d_linear
        for b in range(parts):
            cols = slice(b * width, (b + 1) * width)
            pbuf[g, b] = (against(d_up, wg[cols, :]) + against(d_linear, wu[cols, :])).astype(half)
        for i in range(2):
            start(near_copy(g, 1 - i))

    def far_copy(g):
        return remote(sbuf.at[g], fbuf.at[g], far_sem.at[g], {"tp": far})

    def join_near(g):
        near_copy(g, 1).wait_recv()
        sbuf[g] = (pbuf[g, far].astype(f32) + nbuf[g, 1].astype(f32)).astype(half)
        start(far_copy(g))

    def back_copy(g, i):
        k = g * per + i
        return remote(
            rbuf.at[g, i], ret.at[k], ret_sem.at[k],
            {"sp": lax.rem(me + n - 2 * (k // 2), n) ^ (k % 2)},
        )

    def join_far(g):
        near_copy(g, 0).wait_recv()
        far_copy(g).wait_recv()
        whole = pbuf[g, q].astype(f32) + nbuf[g, 0].astype(f32) + fbuf[g].astype(f32)
        rbuf[g] = whole.astype(half).reshape(per, slots, width)
        for i in range(per):
            if g * per + i > 0:
                start(back_copy(g, i))
        if g == 0:
            ret[0] = whole[:slots].astype(half)

    def grads(h, b):
        some = n // 2
        here = slice(h * some, (h + 1) * some)
        rows = slice(h * some * slots, (h + 1) * some * slots)
        cols = slice(b * width, (b + 1) * width)
        both = over(xbuf[b, here, 0].reshape(some * slots, width), dbuf[rows, :])
        down = over(hbuf[rows, :], xbuf[b, here, 1].reshape(some * slots, width))
        if h == 0:
            acc_g[cols, :] = both[:, :hidden]
            acc_u[cols, :] = both[:, hidden:]
            acc_d[:, cols] = down
        else:
            acc_g[cols, :] += both[:, :hidden]
            acc_u[cols, :] += both[:, hidden:]
            acc_d[:, cols] += down

    def ring_source(j):
        return lax.rem(me + n - 2 * j, n)

    def ring_send(j, source):
        start(remote(mg.at[source], mg.at[source], mx_sem.at[j], {"sp": me ^ 1}))
        if j < lines - 1:
            start(remote(mg.at[source], mg.at[source], mz_sem.at[j + 1], {"sp": lax.rem(me + 2, n)}))

    def ring(j):
        source = ring_source(j)
        spot = mg.at[source]
        if j > 0:
            remote(spot, spot, mz_sem.at[j], {"sp": me ^ 1}).wait_recv()
        ring_send(j, source)

    pl.semaphore_wait(barrier, n + 1)
    ring_start(0)
    for j in range(1, lines):
        start(info_copy(j))
    for copy in loads[2:4]:
        copy.wait()
    arrive(0)

    total = width
    row = lax.broadcasted_iota(jnp.int32, (8, total), 0)

    def forward():
        slow = softplus_of_negative(param_ref[...])
        shift = upright(shift_ref[...])
        for h in range(heads):
            cols = slice(h * head_dim, (h + 1) * head_dim)
            conv = conv_ref[:, cols]
            reset = jax.nn.sigmoid(jnp.dot(conv, wr_ref[h], preferred_element_type=f32))
            inp = jax.nn.sigmoid(jnp.dot(conv, wi_ref[h], preferred_element_type=f32))
            log_decay = -8.0 * reset * slow[:, cols] + shift
            decays = jnp.exp(log_decay)
            norm = jnp.sqrt(-jnp.tanh(log_decay) * (decays * decays + 1.0))
            conv = conv.astype(f32)
            dec[:, cols] = decays
            drive[:, cols] = norm * inp * conv
            fac_o[:, cols] = norm * inp
            fac_i[:, cols] = norm * conv * inp * (1.0 - inp)
            fac_r[:, cols] = (-8.0 * slow[:, cols]) * reset * (1.0 - reset)
            grad[:, cols] = inp * conv * decays * decays / norm

    def forward_scan():
        carry = bs_ref[...]
        for i in range(tokens // 8):
            at = slice(8 * i, 8 * i + 8)
            decay = dec[at, :]
            a = decay
            b = drive[at, :]
            for d in (1, 2, 4):
                b = b + a * jnp.where(row >= d, pltpu.roll(b, d, 0), 0.0)
                a = a * jnp.where(row >= d, pltpu.roll(a, d, 0), 1.0)
            state = a * carry + b
            st[at, :] = state
            prev = jnp.where(row >= 1, pltpu.roll(state, 1, 0), carry)
            fac_r[at, :] = fac_r[at, :] * (decay * prev - grad[at, :])
            carry = state[7:8, :]

    def forward_gate():
        for h in range(heads):
            cols = slice(h * head_dim, (h + 1) * head_dim)
            act, slope = gelu_both(gate_ref[:, cols].astype(f32))
            mg[me, :, cols] = (act * st[:, cols]).astype(half)
            act_b[:, cols] = act
            slope_b[:, cols] = st[:, cols] * slope

    def back_products():
        carry_p = jnp.ones((1, total), f32)
        following = jnp.ones((1, total), f32)
        for i in reversed(range(tokens // 8)):
            at = slice(8 * i, 8 * i + 8)
            decay = dec[at, :]
            a = jnp.where(row < 7, pltpu.roll(decay, 7, 0), following)
            following = decay[0:1, :]
            for d, level in ((1, lev0), (2, lev1), (4, lev2)):
                level[at, :] = jnp.where(row < 8 - d, a, 0.0)
                a = a * jnp.where(row < 8 - d, pltpu.roll(a, 8 - d, 0), 1.0)
            drive[at, :] = a
            p = a * carry_p
            prods[at, :] = p
            carry_p = p[0:1, :]

    for copy in loads[4:11]:
        copy.wait()
    forward()
    forward_scan()
    crossed(0)
    relay(0)
    forward_gate()
    back_products()
    for copy in loads[11:]:
        copy.wait()
    grad_chunks = [functools.partial(grads, h, b) for h in range(2) for b in range(parts)]
    steps = [functools.partial(ring, j) for j in range(lines)]

    def some_of(work, count):
        for _ in range(min(count, len(work))):
            work.pop(0)()

    def ready(count):
        if count % per:
            return
        g = count // per - 1
        expert(g)
        if g == 3:
            join_near(0)
        if g == 5:
            join_near(4)
            join_near(5)

    ready(1)
    for j in range(1, lines):
        arrive(j)
        relay(2 * j - 1)
        if j == max(1, lines - 2):
            some_of(steps, 1)
        ready(2 * j)
        crossed(j)
        if j == lines - 1:
            some_of(steps, 1)
        relay(2 * j)
        ready(2 * j + 1)
    for g in (6, 2, 3):
        join_near(g)
    join_far(4)
    join_far(5)
    relay(n - 1)
    ready(n)
    join_near(7)
    join_near(1)
    for g in (6, 2, 3):
        join_far(g)
    some_of(grad_chunks, 3)
    join_far(7)
    some_of(grad_chunks, 2)
    join_far(0)
    join_far(1)
    some_of(steps, 1)
    some_of(grad_chunks, 3)
    lane = lax.broadcasted_iota(jnp.int32, (tokens, 128), 1)
    away = []
    for j in range(top):
        named = upright(info[0, j : j + 1, :]).astype(jnp.int32)
        gap = lax.shift_right_logical(named, 1) - lax.div(me, 2)
        gap = jnp.where(gap < 0, gap + lines, gap)
        away.append(2 * gap + ((named ^ me) & 1))
    member = jnp.zeros((tokens, 128), f32)
    for j in range(top):
        member = jnp.where(away[j] == lane, 1.0, member)
    earlier = lax.broadcasted_iota(jnp.int32, (tokens, tokens), 1) < (
        lax.broadcasted_iota(jnp.int32, (tokens, tokens), 0)
    )
    rank = jnp.dot(
        jnp.where(earlier, 1.0, 0.0).astype(half), member.astype(half), preferred_element_type=f32
    )
    place = lax.broadcasted_iota(jnp.int32, (tokens, n * slots), 1)
    pick_all = jnp.zeros((tokens, n * slots), f32)
    for j in range(top):
        mine = jnp.sum(jnp.where(away[j] == lane, rank, 0.0), axis=1, keepdims=True)
        pick_all = jnp.where(place == away[j] * slots + mine.astype(jnp.int32), 1.0, pick_all)
    pick_all = pick_all.astype(half)
    for k in range(1, n):
        back_copy(k // per, k % per).wait_recv()
    summed = jnp.dot(pick_all, ret[...].reshape(n * slots, width), preferred_element_type=f32)
    dcols[...] = (cot_ref[...].astype(f32) + summed).astype(half)

    some = n // parts
    thin = width // some
    big, little = tokens // 3, tokens // 6
    owner = lax.div(me, some)
    apart = q ^ owner
    place_in = apart & 1

    def blk_copy(source, i, peer, other, first, size):
        return pltpu.make_async_remote_copy(
            src_ref=source.at[i, first : first + size],
            dst_ref=got.at[me, pl.ds(first, size)],
            send_sem=send_sem.at[1], recv_sem=blk_sem.at[me],
            device_id={"sp": peer, "tp": other}, device_id_type=MESH,
        )

    blocks_sent = []

    def blk_send(source, held, first, size):
        for i in range(some):
            peer = held * some + i
            start(blk_copy(source, i, peer, near, first + size, size))
            mine = blk_copy(source, i, peer, q, first, size)
            blocks_sent.append((peer, mine))

            @pl.when(peer != me)
            def _():
                mine.start()

            @pl.when(peer == me)
            def _():
                got[me, first : first + size] = source[i, first : first + size]

    def rows_big(part):
        return pl.ds(pl.multiple_of(part * big, big), big)

    def rows_little(part):
        return pl.ds(pl.multiple_of(2 * big + part * little, little), little)

    def rows_of(mine, part, inside):
        return rows_big(part) if mine == inside else rows_little(part)

    def got_copy(inside, mine, part, i, other):
        spot = got.at[:, rows_of(mine, part, inside)]
        return pltpu.make_async_remote_copy(
            src_ref=spot, dst_ref=spot, send_sem=send_sem.at[1], recv_sem=got_sem.at[i],
            device_id={"tp": other}, device_id_type=MESH,
        )

    def share(inside):
        spot_rows = rows_of(True, place_in, inside)
        for off in range(1, n):
            source = lax.rem(me + off, n)
            spot = got.at[source, spot_rows]
            remote(spot, spot, blk_sem.at[source], {"tp": far}).wait_recv()

        @pl.when(place_in == 1)
        def _():
            spot = got.at[me, spot_rows]
            remote(spot, spot, blk_sem.at[me], {"tp": far}).wait_recv()

        got_copy(inside, True, place_in, 0, far).start()
        got_copy(inside, True, place_in, 1, near).start()

    def share_on(inside):
        got_copy(inside, False, place_in, 0, far).wait_recv()
        got_copy(inside, False, place_in, 2, near).start()

    def project(inside, mine, part):
        at = rows_of(mine, part, inside)
        count = n * (big if mine == inside else little)
        return over(got[:, at, :].reshape(count, thin), mg[:, at, :].reshape(count, width))

    def project_own(inside):
        go_ref[...] = project(inside, True, place_in)

    def project_rest(inside):
        go_ref[...] += project(inside, False, place_in)
        got_copy(inside, True, place_in ^ 1, 1, near).wait_recv()
        go_ref[...] += project(inside, True, place_in ^ 1)
        got_copy(inside, False, place_in ^ 1, 2, near).wait_recv()
        go_ref[...] += project(inside, False, place_in ^ 1)
        for i, other in ((0, far), (1, near)):
            got_copy(inside, True, place_in, i, other).wait_send()
        got_copy(inside, False, place_in, 2, near).wait_send()

    def each(work, *sides):
        for inside in sides:
            pl.when((apart < 2) == inside)(functools.partial(work, inside))

    def dm_copy(owner, i, other, src):
        return remote(src, dmbuf.at[owner], dm_sem.at[i], {"tp": other})

    start(dm_copy(q, 0, far, dcols))
    start(dm_copy(q, 1, near, dcols))
    for i in range(some):
        bsend[i] = dcols[:, i * thin : (i + 1) * thin]
    blk_send(bsend, q, 0, big)
    while steps:
        steps.pop(0)()
    dmbuf[q] = dcols[...]

    wo_cols = pl.ds(pl.multiple_of(q * width, width), width)
    grad[...] = against(dcols[...], wo[:, wo_cols])
    dm_copy(far, 0, far, dcols).wait_recv()
    start(dm_copy(far, 2, near, dmbuf.at[far]))
    for i in range(some):
        bfar[i, 2 * big :, :] = dmbuf[far, 2 * big :, i * thin : (i + 1) * thin]
    blk_send(bfar, far, 2 * big, little)
    dm_copy(near, 1, near, dcols).wait_recv()
    dm_copy(near ^ 2, 2, near, dcols).wait_recv()
    for shift_by in (1, 2, 3):
        other = q ^ shift_by
        at = pl.ds(pl.multiple_of(other * width, width), width)
        grad[...] += against(dmbuf[other], wo[:, at])
    each(share, True)
    carry = jnp.zeros((1, total), f32)
    for i in reversed(range(tokens // 8)):
        at = slice(8 * i, 8 * i + 8)
        b = grad[at, :]
        gate_out_ref[at, :] = (b * slope_b[at, :]).astype(half)
        b = b * act_b[at, :]
        b = b + lev0[at, :] * pltpu.roll(b, 7, 0)
        b = b + lev1[at, :] * pltpu.roll(b, 6, 0)
        b = b + lev2[at, :] * pltpu.roll(b, 4, 0)
        g = drive[at, :] * carry + b
        grad[at, :] = g
        carry = g[0:1, :]
    first = dec[0:1, :]
    mine_pair[0:1, :] = prods[0:1, :] * first
    mine_pair[1:2, :] = carry * first
    pairs[me] = jnp.zeros((2, total), f32)

    def pair_to(peer, source):
        return remote(mine_pair, pairs.at[source], pair_sem.at[source], {"sp": peer})

    for off in range(1, n):
        start(pair_to(lax.rem(me + off, n), me))
    each(share, False)
    for j in range(lines):
        spot = mg.at[ring_source(j) ^ 1]
        remote(spot, spot, mx_sem.at[j], {"sp": me ^ 1}).wait_recv()
    each(project_own, True, False)
    for off in range(1, n):
        peer = lax.rem(me + off, n)
        pair_to(peer, peer).wait_recv()
    enter = jnp.zeros((1, total), f32)
    each(share_on, True, False)
    for p in reversed(range(n)):
        pair = pairs[p]
        enter = jnp.where(p > me, pair[1:2, :] + pair[0:1, :] * enter, enter)
    for h in range(heads):
        cols = slice(h * head_dim, (h + 1) * head_dim)
        g = grad[:, cols] + prods[:, cols] * enter[:, cols]
        d_r = (g * fac_r[:, cols]).astype(half)
        d_i = (g * fac_i[:, cols]).astype(half)
        out_ref[:, cols] = (
            g * fac_o[:, cols] + against(d_r, wr_ref[h]) + against(d_i, wi_ref[h])
        ).astype(half)
    each(project_rest, True, False)
    for copy in sent:
        copy.wait_send()
    for peer, copy in blocks_sent:

        @pl.when(peer != me)
        def _():
            copy.wait_send()


VM = pl.BlockSpec(memory_space=pltpu.VMEM)


def run_whole(
    n, parts, slots, mixed, cot, ids, weights, conv, gate, bs, param, shift, wr, wi, wg, wu, wd, wo
):
    tokens, width = mixed.shape
    full, hidden = wg.shape
    groups = 8
    per = n // groups
    block = per * slots
    some = n // parts
    thin = width // some
    half, f32 = jnp.bfloat16, jnp.float32
    anywhere = pl.BlockSpec(memory_space=pl.ANY)
    dma, vm = pltpu.SemaphoreType.DMA, pltpu.VMEM
    small = (mixed, cot, ids, weights, conv, gate, bs, param, shift, wr, wi)
    return pl.pallas_call(
        functools.partial(whole_kernel, n, groups),
        out_shape=(
            vm((full, hidden), f32), vm((full, hidden), f32), vm((hidden, full), f32),
            vm((thin, width), f32), vm((tokens, width), half), vm((tokens, width), half),
        ),
        in_specs=[anywhere] * 15,
        out_specs=(VM,) * 6,
        scratch_shapes=[vm(a.shape, a.dtype) for a in small] + [
            vm((full, hidden), half), vm((full, hidden), half), vm((hidden, full), half),
            vm((width, full), half),
            vm((n // 2, 8, tokens), f32),
            vm((min(n // 2, 8), 2, tokens, width), half),
            vm((n // 2, 2, slots, width), half),
            vm((parts, n, 2, slots, width), half),
            vm((n * slots, 2 * hidden), half), vm((n * slots, hidden), half),
            vm((groups, parts, block, width), half),
            vm((groups, 2, block, width), half),
            vm((groups, block, width), half),
            vm((groups, block, width), half),
            vm((groups, per, slots, width), half),
            vm((n, slots, width), half),
            vm((tokens, width), half),
            vm((parts, tokens, width), half),
        ] + [vm((tokens, width), f32)] * 13 + [
            vm((n, tokens, width), half),
            vm((n, tokens, thin), half),
            vm((some, tokens, thin), half),
            vm((some, tokens, thin), half),
            vm((2, width), f32),
            vm((n, 2, width), f32),
            dma((2,)), dma((n // 2, 2)), pltpu.SemaphoreType.REGULAR, dma((n // 2, 2)), dma((n // 2,)), dma((n // 2,)), dma((n,)), dma((n,)), dma((n,)),
            dma((groups, 2)),
            dma((groups,)), dma((n,)), dma((3,)), dma((15,)),
            dma((n // 2,)), dma((n // 2,)), dma((n,)), dma((3,)), dma((n,)),
        ],
        compiler_params=pltpu.CompilerParams(
            collective_id=0, has_side_effects=True, vmem_limit_bytes=57000 * 1024
        ),
        cost_estimate=pl.CostEstimate(flops=8_000_000_000, bytes_accessed=80_000_000, transcendentals=0),
    )(mixed, cot, ids, weights, conv, gate, bs, param, shift, wr, wi, wg, wu, wd, wo)


def write_kernel(*refs):
    count = len(refs) // 2
    copies = [
        pltpu.make_async_copy(refs[i], refs[count + i], refs[-1].at[i]) for i in range(count)
    ]
    for copy in copies:
        copy.start()
    for copy in copies:
        copy.wait()


def write_out(*arrays):
    held = [pltpu.with_memory_space_constraint(a, pltpu.VMEM) for a in arrays]
    return pl.pallas_call(
        write_kernel,
        out_shape=tuple(jax.ShapeDtypeStruct(a.shape, a.dtype) for a in arrays),
        in_specs=[VM] * len(arrays),
        out_specs=(pl.BlockSpec(memory_space=pl.ANY),) * len(arrays),
        scratch_shapes=[pltpu.SemaphoreType.DMA((len(arrays),))],
        compiler_params=pltpu.CompilerParams(vmem_limit_bytes=1024 * 1024),
    )(*held)


def body(
    conv_out, gate_in, block_states, decay_param, decay_shift, w_reset, w_input, w_out,
    mixed, d_out, expert_ids, route_weights, w_gate, w_up, w_down,
):
    tok_rows, top_k = expert_ids.shape
    experts = lax.axis_size("sp")
    capacity = 2 * tok_rows * top_k // experts
    slots = -(-capacity // 16) * 16
    results = run_whole(
        experts, lax.axis_size("tp"), slots, mixed, d_out, expert_ids.T, route_weights.T,
        conv_out, gate_in, block_states, decay_param[None, :], decay_shift[None, :],
        w_reset, w_input, w_gate[0], w_up[0], w_down[0], w_out,
    )
    grad_gate_e, grad_up_e, grad_down_e, grad_out, grad_in, grad_gate = write_out(*results)
    return (grad_gate_e[None], grad_up_e[None], grad_down_e[None], grad_out, grad_in, grad_gate)


def solution(mesh):
    placed = (
        P("sp", "tp"),
        P("sp", "tp"),
        P("sp", "tp"),
        P("tp"),
        P("sp"),
        P("tp", None, None),
        P("tp", None, None),
        P("tp", None),
        P("sp", "tp"),
        P("sp", "tp"),
        P("sp", None),
        P("sp", None),
        P("sp", None, "tp"),
        P("sp", None, "tp"),
        P("sp", "tp", None),
    )
    return jax.shard_map(
        body,
        mesh=mesh,
        in_specs=placed,
        out_specs=(
            P("sp", None, "tp"),
            P("sp", None, "tp"),
            P("sp", "tp", None),
            P("sp", "tp"),
            P("sp", "tp"),
            P("sp", "tp"),
        ),
        check_vma=False,
    )
```
